512 devices in a mesh: ep: 128 (over z, y, core), tp: 4 (over x).
Axes of the slice: x: 4, y: 8, z: 8, core: 2. Of those that a mesh axis runs over, the one named last changes fastest.
Arguments:
- tokens: bfloat16 [384, 2048], P('ep'), may hold values from -6 to 6
- mixer_gain: float32 [2048], replicated, may hold values from 0.1 to 1.9
- query_weight: bfloat16 [2048, 2048], P('ep', 'tp'), may hold values from -0.125 to 0.125
- key_cache: bfloat16 [384, 1024, 4, 128], P('ep', None, 'tp'), may hold values from -6 to 6
- value_cache: bfloat16 [384, 1024, 4, 128], P('ep', None, 'tp'), may hold values from -6 to 6
- seq_lengths: int32 [384], P('ep'), may hold values from 1 to 1024, as said below
- head_offset: float32 [16], P('tp'), may hold values from -8.5 to -3.5
- output_weight: bfloat16 [2048, 2048], P('tp', 'ep'), may hold values from -0.5 to 0.5
- expert_gain: float32 [2048], replicated, may hold values from 0.1 to 1.9
- expert_ids: int32 [384, 2], P('ep'), may hold values from 0 to 127, as said below
- route_weight: float32 [384, 2], P('ep'), may hold values from 0.2 to 1
- gate_weight: bfloat16 [128, 2048, 1024], P('ep', None, 'tp'), may hold values from -0.125 to 0.125
- up_weight: bfloat16 [128, 2048, 1024], P('ep', None, 'tp'), may hold values from -0.125 to 0.125
- down_weight: bfloat16 [128, 1024, 2048], P('ep', 'tp'), may hold values from -0.1875 to 0.1875
Outputs:
- layer_out: bfloat16 [384, 2048], P('ep', 'tp')
The draws below stay inside these ranges and needn't reach their ends.
Inputs may be any that keep to these rules, and one draw needn't show every extreme that they name: `seq_lengths`: some sequence holds all 1024 positions. `expert_ids`: the 2 experts of a row are different and lie in one group of 4 consecutive expert numbers. Among the 3 rows of one index of ep no expert is named by more than 2 rows, and some expert by exactly 2.
All inputs are finite; a program needn't handle non-finite values.
Results may differ from the reference program's by a relative error of at most 0.012.
Values may be sent and summed in bfloat16 or wider, within the bound.
A program may use at most 64 MiB of HBM per device.

```python
import jax
import jax.numpy as jnp
from jax import lax

D = 2048
HEADS = 16
KV_HEADS = 4
HD = 128
FF_E = 1024
EPG = 4
TOP = 2
CACHE = 1024
B_DEV = 3
B_TOT = 384
EXPERTS = 128
GROUPS = 32
CAP = 2
N_TP = 4


def draw_seq_lengths(key, part):
    first = jax.random.randint(jax.random.fold_in(key, 11), (B_TOT,), 1, CACHE + 1)
    second = jax.random.randint(jax.random.fold_in(key, 12), (B_TOT,), 1, CACHE + 1)
    chosen = jax.random.randint(jax.random.fold_in(key, 13), (), 0, B_TOT)
    lengths = jnp.minimum(first, second)
    lengths = jnp.where(jnp.arange(B_TOT) == chosen, CACHE, lengths)
    return lengths.astype(jnp.int32)


def draw_expert_ids(key, part):
    blocks = B_TOT // B_DEV
    group_keys = jax.random.split(jax.random.fold_in(key, 21), blocks)
    group_order = jax.vmap(lambda single: jax.random.permutation(single, GROUPS))(group_keys)
    sets = jnp.arange(B_DEV) // CAP
    groups = group_order[:, sets]
    leads = jax.random.randint(jax.random.fold_in(key, 22), (blocks, GROUPS), 0, EPG)[:, sets]
    other_keys = jax.random.split(jax.random.fold_in(key, 23), blocks * B_DEV)
    others = jax.vmap(lambda single: jax.random.permutation(single, EPG - 1))(other_keys)[:, :TOP - 1] + 1
    others = others.reshape(blocks, B_DEV, TOP - 1)
    inside = jnp.concatenate([leads[:, :, None], (leads[:, :, None] + others) % EPG], axis=2)
    numbers = groups[:, :, None] * EPG + inside
    return numbers.reshape(B_TOT, TOP).astype(jnp.int32)


def block_scale(rng, extent, cuts, smallest, largest):
    loudness, own = 1.0, jax.random.fold_in(rng, 6)
    for axis_at, shards_of in cuts:
        steps = jnp.exp(jax.random.uniform(jax.random.fold_in(own, axis_at), (shards_of,), jnp.float32, smallest / len(cuts), largest / len(cuts)))
        loudness = loudness * jnp.repeat(steps, extent[axis_at] // shards_of).reshape([-1 if axis == axis_at else 1 for axis in range(len(extent))])
    return loudness


def normal_values(key, shape, deviation, most, shards=(), kind=jnp.bfloat16):
    array = jax.random.normal(key, shape, jnp.float32) * deviation
    if len(shards) > 0:
        array = block_scale(key, shape, shards, -0.22, 0.18) * array
    return jnp.clip(array, min=-most, max=most).astype(kind)


def setup_inputs(seed: int = 0) -> dict:
    seeds = jax.random.split(jax.random.key(seed), 15)
    return {
        "tokens": normal_values(seeds[0], (B_TOT, D), 1.0, 6.0, ((0, 128),)),
        "mixer_gain": jnp.clip(1.0 + 0.18 * jax.random.normal(seeds[1], (D,), jnp.float32), 0.1, 1.9),
        "query_weight": normal_values(seeds[2], (D, HEADS * HD), D ** -0.5, 0.125, ((0, 128), (1, 4))),
        "key_cache": normal_values(seeds[3], (B_TOT, CACHE, KV_HEADS, HD), 1.0, 6.0, ((0, 128), (2, 4))),
        "value_cache": normal_values(seeds[4], (B_TOT, CACHE, KV_HEADS, HD), 1.0, 6.0, ((0, 128), (2, 4))),
        "seq_lengths": draw_seq_lengths(jax.random.fold_in(seeds[14], 71), 0),
        "head_offset": jnp.clip(-8.5 + 5.0 * jax.random.uniform(seeds[6], (HEADS,), jnp.float32) ** block_scale(seeds[6], (HEADS,), ((0, 4),), -0.2, 0.2), -8.5, -3.5),
        "output_weight": normal_values(seeds[7], (HEADS * HD, D), HD ** -0.5, 0.5, ((0, 4), (1, 128))),
        "expert_gain": jnp.clip(1.0 + 0.18 * jax.random.normal(seeds[8], (D,), jnp.float32), 0.1, 1.9),
        "expert_ids": draw_expert_ids(jax.random.fold_in(seeds[14], 71), 0),
        "route_weight": jnp.clip(0.2 + 0.8 * jax.random.uniform(seeds[10], (B_TOT, TOP), jnp.float32) ** block_scale(seeds[10], (B_TOT, TOP), ((0, 128),), -0.2, 0.2), 0.2, 1.0),
        "gate_weight": normal_values(seeds[11], (EXPERTS, D, FF_E), D ** -0.5, 0.125, ((0, 128), (2, 4))),
        "up_weight": normal_values(seeds[12], (EXPERTS, D, FF_E), D ** -0.5, 0.125, ((0, 128), (2, 4))),
        "down_weight": normal_values(seeds[13], (EXPERTS, FF_E, D), FF_E ** -0.5, 0.1875, ((0, 128), (1, 4))),
    }


def rms_norm(values, gain):
    wide = values.astype(jnp.float32)
    scale = lax.rsqrt(lax.optimization_barrier(jnp.mean(wide * wide, axis=-1, keepdims=True)) + 1e-06)
    return (wide * scale * gain).astype(jnp.bfloat16)

def reference(tokens, mixer_gain, query_weight, key_cache, value_cache, seq_lengths, head_offset, output_weight, expert_gain, expert_ids, route_weight, gate_weight, up_weight, down_weight):
    normed = rms_norm(tokens, mixer_gain)
    query = jnp.dot(normed, query_weight, preferred_element_type=jnp.float32).astype(jnp.bfloat16)
    per_group = HEADS // KV_HEADS
    scale = HD ** (-0.5)
    offset = head_offset.reshape(KV_HEADS, per_group, 1)

    def attend(args):
        query_row, keys, values, length = args
        grouped = query_row.reshape(KV_HEADS, per_group, HD).astype(jnp.float32)
        score = jnp.einsum('kgd,skd->kgs', grouped, keys.astype(jnp.float32)) * scale + offset
        valid = (jnp.arange(CACHE, dtype=jnp.int32) < length)[None, None, :]
        log_take = jax.nn.log_sigmoid(score)
        log_pass = jnp.where(valid, jax.nn.log_sigmoid(-score), 0.0)
        later = lax.cumsum(log_pass, axis=2, reverse=True) - log_pass
        weight = jnp.where(valid, jnp.exp(log_take + later), 0.0).astype(jnp.bfloat16)
        result = jnp.einsum('kgs,skd->kgd', weight.astype(jnp.float32), values.astype(jnp.float32))
        return result.reshape(HEADS * HD).astype(jnp.bfloat16)
    mixed = lax.map(attend, (query, key_cache, value_cache, seq_lengths))
    quarter_width = HEADS * HD // N_TP
    total = tokens.astype(jnp.float32)
    for quarter in range(N_TP):
        part = jnp.dot(mixed[:, quarter * quarter_width:(quarter + 1) * quarter_width], output_weight[quarter * quarter_width:(quarter + 1) * quarter_width], preferred_element_type=jnp.float32).astype(jnp.bfloat16)
        total = total + lax.optimization_barrier(part).astype(jnp.float32)
    resid = total.astype(jnp.bfloat16)
    normed2 = rms_norm(resid, expert_gain)
    flat_ids = expert_ids.reshape(-1).astype(jnp.int32)
    row_ids = (jnp.arange(B_TOT * TOP, dtype=jnp.int32) // TOP).astype(jnp.int32)
    unit_width = FF_E // N_TP

    def expert(args):
        number, row_index = args
        row = lax.dynamic_slice_in_dim(normed2, row_index, 1, 0)
        gate = jnp.dot(row, gate_weight[number], preferred_element_type=jnp.float32)
        upward = jnp.dot(row, up_weight[number], preferred_element_type=jnp.float32)
        hidden = (jax.nn.silu(gate) * upward).astype(jnp.bfloat16)
        downs = down_weight[number]
        summed = jnp.zeros((1, D), jnp.float32)
        for quarter in range(N_TP):
            part = jnp.dot(hidden[:, quarter * unit_width:(quarter + 1) * unit_width], downs[quarter * unit_width:(quarter + 1) * unit_width], preferred_element_type=jnp.float32).astype(jnp.bfloat16)
            summed = summed + lax.optimization_barrier(part).astype(jnp.float32)
        return summed.astype(jnp.bfloat16)[0]
    outputs = lax.map(expert, (flat_ids, row_ids))
    weighted = outputs.reshape(B_TOT, TOP, D).astype(jnp.float32) * route_weight[:, :, None]
    return (resid.astype(jnp.float32) + lax.optimization_barrier(jnp.sum(weighted, axis=1))).astype(jnp.bfloat16)
```

```python
import functools
from types import SimpleNamespace

import jax
import jax.numpy as jnp
from jax import lax
from jax.experimental import pallas as pl
from jax.experimental.pallas import tpu as pltpu
from jax.sharding import Mesh
from jax.sharding import PartitionSpec as P

EP = ("z", "y", "c")
SLOTS = 16
PAD = 4
F32 = jnp.float32
BF16 = jnp.bfloat16


def iota(shape, dim):
    return lax.broadcasted_iota(jnp.int32, shape, dim)


def dot(a, b, dims=((1,), (0,)), precision=None):
    return lax.dot_general(a, b, (dims, ((), ())), precision=precision, preferred_element_type=F32)


def onehot(condition):
    return jnp.where(condition, 1.0, 0.0).astype(BF16)


def near_first(count):
    return sorted(range(1, count), key=lambda k: min(k, count - k))


def far_first(count):
    return near_first(count)[::-1]


def stacked(ref, count):
    return jnp.concatenate([ref[t].astype(F32) for t in range(count)], axis=0).astype(BF16)


def remote(src, dst, send_sem, recv_sem, **where):
    return pltpu.make_async_remote_copy(
        src_ref=src,
        dst_ref=dst,
        send_sem=send_sem,
        recv_sem=recv_sem,
        device_id=where,
        device_id_type=pl.DeviceIdType.MESH,
    )


def attention(d, q, kbuf, vbuf, lens, hoff):
    heads = d.ql // d.hd
    rows = heads * 8
    queries = jnp.concatenate([q[:, h * d.hd : (h + 1) * d.hd] for h in range(heads)], axis=0)
    queries = queries.astype(BF16)
    row = iota((rows, 1), 0)
    seq = row & 7
    head = row >> 3
    score = jnp.zeros((rows, d.cache), F32)
    length = jnp.zeros((rows, 1), jnp.int32)
    offset = jnp.zeros((rows, 1), F32)
    for b in range(d.b):
        one = dot(queries, kbuf[b], ((1,), (1,)))
        score = jnp.where(seq == b, one, score)
        length = jnp.where(seq == b, lens[b], length)
    for h in range(heads):
        offset = jnp.where(head == h, hoff[h], offset)
    score = score * (d.hd**-0.5) + offset
    valid = iota((rows, d.cache), 1) < length
    soft = jnp.log1p(jnp.exp(-jnp.abs(score)))
    log_take = jnp.minimum(score, 0.0) - soft
    log_pass = jnp.where(valid, jnp.minimum(-score, 0.0) - soft, 0.0)
    blocks = d.cache // 128
    pieces = [log_pass[:, i * 128 : (i + 1) * 128] for i in range(blocks)]
    after = (iota((128, 128), 0) > iota((128, 128), 1)).astype(F32)
    inside = dot(jnp.concatenate(pieces, axis=0), after, precision=lax.Precision.HIGHEST)
    later = jnp.zeros((rows, 1), F32)
    sums = [None] * blocks
    for i in range(blocks - 1, -1, -1):
        sums[i] = inside[i * rows : (i + 1) * rows] + later
        later = later + jnp.sum(pieces[i], axis=1, keepdims=True)
    weight = jnp.where(valid, jnp.exp(log_take + jnp.concatenate(sums, axis=1)), 0.0).astype(BF16)
    total = jnp.zeros((rows, d.hd), F32)
    for b in range(d.b):
        total = jnp.where(seq == b, dot(weight, vbuf[b]), total)
    return jnp.concatenate([total[h * 8 : (h + 1) * 8] for h in range(heads)], axis=1).astype(BF16)


def kernel(d, *refs):
    (tokens_in, mgain_in, wq_in_hbm, key, val, lens_in, hoff_in, wo_in_hbm, egain_in, ids_in, rw_in,
     gate, up, down) = refs[:14]
    out, line_out, info_out, most_out = refs[14:18]
    (tokens, mgain, wq, wo, egain, lens, hoff, ids, rw,
     kbuf, vbuf, gbuf, ubuf, dbuf, load_sem,
     ta_send, ta_recv, qa_send, qa_recv, wq_all, wo_all, qp_send, qp_recv, mx_send, mx_recv,
     pt_send, pt_recv, rb_send, line_rows, own_send, rows, s_send, s_recv, h_send, h_recv,
     y_send, y_recv, z_send, z_recv,
     info_a, info_az, info_b, info_by, info_c, info_cc,
     zs, zr, ys, yr, xs, xr, cs, cr) = refs[18:]
    z, y, c, x = (lax.axis_index(name) for name in ("z", "y", "c", "x"))
    nz, ny, nc, nx, b = d.nz, d.ny, d.nc, d.nx, d.b
    other = 1 - c
    slot = c * ny + y
    line = nz * b
    home = z // d.nb
    MESH = pl.DeviceIdType.MESH

    def up_z(k):
        return lax.rem(z + k, nz)

    def up_y(k):
        return lax.rem(y + k, ny)

    def up_x(k):
        return lax.rem(x + k, nx)

    def up_c(k):
        return lax.rem(c + k, nc)

    small = [
        pltpu.make_async_copy(src, dst, load_sem.at[14 + i])
        for i, (src, dst) in enumerate([
            (tokens_in, tokens), (mgain_in, mgain), (wq_in_hbm, wq), (ids_in, ids), (rw_in, rw),
            (wo_in_hbm, wo), (lens_in, lens), (hoff_in, hoff), (egain_in, egain),
        ])
    ]
    for copy in small:
        copy.start()
    barrier = pltpu.get_barrier_semaphore()
    peers = [{"z": up_z(k), "c": up_c(j)} for k in far_first(nz) for j in range(nc)]
    peers += [{"y": up_y(k)} for k in far_first(ny)]
    peers += [{"x": up_x(k), "c": up_c(j)} for k in far_first(nx) for j in range(nc)]
    peers += [{"c": other}]
    for peer in peers:
        pl.semaphore_signal(barrier, inc=1, device_id=peer, device_id_type=MESH)

    loads = [
        pltpu.make_async_copy(src, dst, load_sem.at[i])
        for i, (src, dst) in enumerate(
            [(key, kbuf), (val, vbuf), (gate, gbuf), (up, ubuf), (down, dbuf)]
        )
    ]
    for copy in loads:
        copy.start()
    for copy in small:
        copy.wait()

    wide = tokens[...].astype(F32)
    scale = lax.rsqrt(jnp.mean(wide * wide, axis=1, keepdims=True) + 1e-06)
    normed = (wide * scale * mgain[...]).astype(BF16).astype(F32)
    filler = jnp.zeros((PAD - b, d.width), F32)
    normed = jnp.concatenate([normed, filler], axis=0)
    plain = jnp.concatenate([wide, filler], axis=0).astype(BF16)
    for t in range(nz):
        ta_send[t] = plain[:, t * d.zb : (t + 1) * d.zb]
    share = ny * d.rp
    depth, tall = d.rp.bit_length() - 1, share.bit_length() - 1
    to = iota((d.zb, d.zb), 1)
    source = ((((to & (share - 1)) >> depth) * nc + (to >> tall)) << depth) + (to & (d.rp - 1))
    order = onehot(iota((d.zb, d.zb), 0) == source)
    moved = dot(
        jnp.concatenate([normed[:, t * d.zb : (t + 1) * d.zb] for t in range(nz)], axis=0).astype(BF16),
        order).astype(BF16)
    for t in range(nz):
        for j in range(nc):
            qa_send[t * nc + j] = moved[t * PAD : (t + 1) * PAD, j * share : (j + 1) * share]
    lane = iota((8, d.nt), 1)
    field = iota((8, d.nt), 0)
    info = jnp.zeros((8, d.nt), F32)
    for r in range(b):
        here = lane == slot * line + z * b + r
        for j, number in enumerate((
            ids[0, r].astype(F32), ids[1, r].astype(F32), rw[0, r], rw[1, r],
        )):
            info = jnp.where(here & (field == j), number, info)
    info_a[...] = info
    pl.semaphore_wait(barrier, len(peers))

    pending = []

    def send(copy):
        copy.start()
        pending.append(copy)
        return copy

    def keep(number, src, dst):
        copy = pltpu.make_async_copy(src, dst, load_sem.at[number])
        copy.start()
        return copy

    zc = [(k, j) for k in far_first(nz) for j in range(nc)] + [(0, j) for j in range(1, nc)]
    me = z * nc + c

    def there(k, j):
        return up_z(k) * nc + up_c(j)

    def zc_exchange(base, source, everything):
        return [
            send(remote(
                source.at[there(k, j)], everything.at[me],
                zs.at[base + k * nc + j], zr.at[base + k * nc + j], z=up_z(k), c=up_c(j)))
            for k, j in zc
        ]

    own_rows = pl.multiple_of(y * d.rp, 8)
    own_piece = pl.multiple_of((y * nc + c) * d.rp, 8)

    def from_y(k):
        return lax.rem(y - k + ny, ny)

    wq_in = [
        send(remote(wq, wq_all.at[pl.ds(own_rows, d.rp)], ys.at[k], yr.at[k], y=up_y(k)))
        for k in far_first(ny)
    ]
    own_q = keep(5, wq, wq_all.at[pl.ds(own_rows, d.rp)])
    qa_in = zc_exchange(0, qa_send, qa_recv)
    own_a = keep(7, qa_send.at[me], qa_recv.at[me])
    info_in = [
        send(remote(info_a, info_az.at[z], zs.at[4 * nz + k], zr.at[4 * nz + k], z=up_z(k)))
        for k in far_first(nz)
    ]
    wo_in = {
        k: send(remote(wo, wo_all.at[pl.ds(own_piece, d.rp)], ys.at[ny + k], yr.at[ny + k], y=up_y(k)))
        for k in far_first(ny)
    }
    own_o = keep(6, wo, wo_all.at[pl.ds(own_piece, d.rp)])
    wo_fwd = [send(remote(wo, wo_all.at[pl.ds(own_piece, d.rp)], cs.at[0], cr.at[0], c=other))]
    ta_in = [
        send(remote(ta_send.at[up_z(k)], ta_recv.at[z], zs.at[5 * nz + k], zr.at[5 * nz + k], z=up_z(k)))
        for k in far_first(nz)
    ]
    own_t = keep(8, ta_send.at[z], ta_recv.at[z])

    for copy in qa_in:
        copy.wait_recv()
    own_a.wait()
    own_q.wait()
    rows_a = stacked(qa_recv, nz * nc)
    for copy in wq_in:
        copy.wait_recv()
    partial = dot(rows_a, wq_all[...]).astype(BF16)
    for t in range(nz * nc):
        qp_send[t] = partial[t * PAD : (t + 1) * PAD]
    qp_in = zc_exchange(2 * nz, qp_send, qp_recv)
    own_p = keep(9, qp_send.at[me], qp_recv.at[me])

    for k in near_first(ny):
        wo_in[k].wait_recv()
        part = wo_all.at[pl.ds(pl.multiple_of((from_y(k) * nc + c) * d.rp, 8), d.rp)]
        wo_fwd.append(send(remote(part, part, cs.at[k], cr.at[k], c=other)))
    for copy in info_in:
        copy.wait_recv()
    info = info_a[...]
    for k in range(1, nz):
        info = info + info_az[up_z(k)]
    info_b[...] = info
    info_y_in = [
        send(remote(info_b, info_by.at[y], ys.at[2 * ny + k], yr.at[2 * ny + k], y=up_y(k)))
        for k in far_first(ny)
    ]
    loads[0].wait()
    loads[1].wait()

    for copy in qp_in:
        copy.wait_recv()
    own_p.wait()
    q = qp_recv[0].astype(F32)
    for t in range(1, nz * nc):
        q = q + qp_recv[t].astype(F32)
    q = jnp.concatenate([q, jnp.zeros((8 - PAD, d.ql), F32)], axis=0)
    mixed = attention(d, q, kbuf, vbuf, lens, hoff)
    mx_send[...] = mixed[0:PAD]
    mx_in = [
        send(remote(mx_send, mx_recv.at[z], zs.at[6 * nz + k], zr.at[6 * nz + k], z=up_z(k)))
        for k in far_first(nz)
    ]
    own_m = keep(10, mx_send, mx_recv.at[z])

    for copy in info_y_in:
        copy.wait_recv()
    info = info_b[...]
    for k in range(1, ny):
        info = info + info_by[up_y(k)]
    info_c[...] = info
    info_c_in = send(remote(info_c, info_cc, cs.at[ny], cr.at[ny], c=other))

    pick_t = iota((line, nz * PAD), 0)
    pick_s = iota((line, nz * PAD), 1)
    within = pick_s & (PAD - 1)
    pick = onehot((within < b) & ((pick_s >> (PAD.bit_length() - 1)) * b + within == pick_t))
    for copy in ta_in:
        copy.wait_recv()
    own_t.wait()
    tok = dot(pick, stacked(ta_recv, nz))
    for copy in wo_fwd:
        copy.wait_recv()
    own_o.wait()
    for copy in mx_in:
        copy.wait_recv()
    own_m.wait()
    tight = dot(pick, stacked(mx_recv, nz)).astype(BF16)
    part = dot(tight, wo_all[...], ((1,), (1,)))
    pt_send[...] = part.astype(BF16)

    away = remote(pt_send, pt_recv.at[x], xs.at[0], xr.at[x], x=home)
    own_lanes = pl.multiple_of(lax.rem(z, d.nb) * d.zb, d.zb)
    own_block = line_rows.at[:, pl.ds(own_lanes, d.zb)]
    own_b = pltpu.make_async_copy(rb_send, own_block, load_sem.at[11])

    def to_line(k):
        return remote(
            rb_send, own_block, zs.at[7 * nz + k], zr.at[7 * nz + lax.rem(z, d.nb)], z=up_z(k))

    @pl.when(x != home)
    def _():
        away.start()

    @pl.when(x == home)
    def _():
        total = tok + pt_send[...].astype(F32)
        for k in range(1, nx):
            source = lax.rem(x + k, nx)
            remote(pt_send, pt_recv.at[source], xs.at[0], xr.at[source], x=source).wait_recv()
            total = total + pt_recv[source].astype(F32)
        rb_send[...] = total.astype(BF16)
        own_b.start()
        for k in far_first(nz):
            to_line(k).start()

    info_c_in.wait_recv()
    info = info_c[...] + info_cc[...]
    info_out[...] = info
    id0 = info[0:1]
    id1 = info[1:2]
    count = float(ny * nc)
    low = z.astype(F32) * count
    half_width = ny * line

    def line_of(places):
        return jnp.floor((places.astype(F32) + 0.5) * (1.0 / line))

    token_line = line_of(iota((1, d.nt), 1))
    token_half = jnp.where(token_line >= ny, 1.0, 0.0)
    ours = token_half == c.astype(F32)
    staying = (id0 >= low) & (id0 < low + count)
    stay = jnp.where(staying, 1.0, 0.0)
    hits = []
    for j in range(nc):
        expert = low + (y * nc + j).astype(F32)
        hits.append((jnp.where(id0 == expert, 1.0, 0.0), jnp.where(id1 == expert, 1.0, 0.0)))
    first, second = iota((d.nt, d.nt), 0), iota((d.nt, d.nt), 1)
    earlier = first < second
    same_line = line_of(first) == line_of(second)
    same_half = (first < half_width) == (second < half_width)
    line_rank = dot(jnp.broadcast_to(stay, (8, d.nt)).astype(BF16), onehot(earlier & same_line))[0:1]
    hit_rows = jnp.concatenate([h0 + h1 for h0, h1 in hits], axis=0)
    hit_rank = dot(hit_rows.astype(BF16), onehot(earlier & same_half))
    numbers = iota((SLOTS, d.nt), 0).astype(F32)
    chosen = [
        onehot((numbers == hit_rank[j : j + 1]) & (hit_rows[j : j + 1] > 0.5) & ours) for j in range(nc)
    ]
    routes = [h0 * info[2:3] + h1 * info[3:4] for h0, h1 in hits]
    slot_route = jnp.concatenate([
        jnp.sum(chosen[j].astype(F32) * routes[j], axis=1, keepdims=True) for j in range(nc)], axis=0)
    chosen = jnp.concatenate(chosen, axis=0)
    kept = ny * SLOTS
    place = (token_line - c.astype(F32) * ny) * SLOTS + line_rank
    packed = onehot(
        (iota((kept, d.nt), 0).astype(F32) == place) & staying & ours & (line_rank < SLOTS - 0.5))
    chosen = dot(chosen, packed, ((1,), (1,))).astype(BF16)
    own_token = onehot(iota((d.nt, line), 0) == iota((d.nt, line), 1) + slot * line)
    own_pack = dot(
        onehot((numbers == line_rank) & staying & (token_line == slot.astype(F32))), own_token).astype(BF16)
    spread_s = iota((nz * 8, line), 0)
    spread_t = iota((nz * 8, line), 1)
    spread = onehot(((spread_s & 7) < b) & ((spread_s >> 3) * b + (spread_s & 7) == spread_t))
    spread = dot(spread, own_pack, ((1,), (1,))).astype(BF16)
    expert = iota((d.experts, d.nt), 0).astype(F32)
    named = onehot((id0 == expert) | (id1 == expert))
    group_t = iota((d.nt, 128), 0)
    group_g = iota((d.nt, 128), 1)
    halves = dot(named, onehot((group_t >= half_width) == (group_g > 0)))
    zone = iota((8, d.nt), 0).astype(F32) * count
    lines = dot(onehot((id0 >= zone) & (id0 < zone + count)), onehot(line_of(group_t) == group_g.astype(F32)))
    most = jnp.maximum(jnp.max(halves), jnp.max(lines))
    most_out[0] = jnp.where(most > SLOTS, 1, 0)

    for j in range(d.nb):
        source = x * d.nb + j

        @pl.when(z != source)
        def _():
            block = line_rows.at[:, pl.ds(j * d.zb, d.zb)]
            remote(rb_send, block, zs.at[0], zr.at[7 * nz + j], z=source).wait_recv()

    @pl.when(x == home)
    def _():
        own_b.wait()

    save = keep(12, line_rows, line_out)
    own_send[...] = dot(own_pack, line_rows[...]).astype(BF16)
    own_slots = pl.ds(pl.multiple_of(y * SLOTS, SLOTS), SLOTS)
    rows_in = [
        send(remote(own_send, rows.at[own_slots], ys.at[3 * ny + k], yr.at[3 * ny + k], y=up_y(k)))
        for k in far_first(ny)
    ]
    own_s = keep(13, own_send, rows.at[own_slots])
    mine_t = iota((8, line), 1)
    mine_r = iota((8, line), 0)
    resid = dot(onehot((mine_r < b) & (mine_t == mine_r + z * b)), line_rows[...])
    own_s.wait()
    for copy in rows_in:
        copy.wait_recv()

    s_send[...] = dot(chosen, rows[...]).astype(BF16).reshape(nc, SLOTS, d.xs)
    xc = [(k, j) for k in far_first(nx) for j in range(nc)] + [(0, j) for j in range(1, nc)]
    our_slots = pl.ds(pl.multiple_of(c * SLOTS, SLOTS), SLOTS)
    s_in = [
        send(remote(
            s_send.at[up_c(j)], s_recv.at[x, our_slots],
            xs.at[1 + k * nc + j], xr.at[nx + k * nc + j], x=up_x(k), c=up_c(j)))
        for k, j in xc
    ]
    own_s = keep(5, s_send.at[c], s_recv.at[x, our_slots])
    for copy in loads[2:]:
        copy.wait()
    own_s.wait()
    for copy in s_in:
        copy.wait_recv()
    wide = [s_recv[t].astype(F32) for t in range(nx)]
    square = sum(jnp.sum(part * part, axis=1, keepdims=True) for part in wide)
    scale = lax.rsqrt(square / d.width + 1e-06)
    gated = jnp.zeros((nc * SLOTS, d.ff), F32)
    upward = jnp.zeros((nc * SLOTS, d.ff), F32)
    for t in range(nx):
        span = slice(t * d.xs, (t + 1) * d.xs)
        part = (wide[t] * scale * egain[:, span]).astype(BF16)
        gated = gated + dot(part, gbuf[span, :])
        upward = upward + dot(part, ubuf[span, :])
    hidden = (gated / (1.0 + jnp.exp(-gated)) * upward).astype(BF16)
    for t in range(nx):
        h_send[t] = dot(hidden, dbuf[:, t * d.xs : (t + 1) * d.xs]).astype(BF16)

    def to_half(j):
        return pl.ds(pl.multiple_of(up_c(j) * SLOTS, SLOTS), SLOTS)

    h_in = [
        send(remote(
            h_send.at[up_x(k), to_half(j)], h_recv.at[x, our_slots],
            xs.at[1 + nx * nc + k * nc + j], xr.at[nx + nx * nc + k * nc + j], x=up_x(k), c=up_c(j)))
        for k, j in xc
    ]
    own_h = keep(6, h_send.at[x, our_slots], h_recv.at[x, our_slots])
    own_h.wait()
    for copy in h_in:
        copy.wait_recv()
    total = h_recv[0].astype(F32)
    for t in range(1, nx):
        total = total + h_recv[t].astype(F32)
    answer = (total.astype(BF16).astype(F32) * slot_route).astype(BF16)
    y_send[...] = dot(chosen, answer, ((0,), (0,))).astype(BF16).reshape(ny, SLOTS, d.xs)
    y_in = [
        send(remote(y_send.at[up_y(k)], y_recv.at[y], ys.at[4 * ny + k], yr.at[4 * ny + k], y=up_y(k)))
        for k in far_first(ny)
    ]
    own_y = keep(7, y_send.at[y], y_recv.at[y])
    own_y.wait()
    for copy in y_in:
        copy.wait_recv()
    total = y_recv[0].astype(F32)
    for t in range(1, ny):
        total = total + y_recv[t].astype(F32)
    owned = dot(spread, total.astype(BF16)).astype(BF16)
    for t in range(nz):
        z_send[t] = owned[t * 8 : t * 8 + PAD]
    z_in = [
        send(remote(z_send.at[up_z(k)], z_recv.at[z], zs.at[8 * nz + k], zr.at[8 * nz + k], z=up_z(k)))
        for k in far_first(nz)
    ]
    own_z = keep(8, z_send.at[z], z_recv.at[z])
    save.wait()

    @pl.when(x != home)
    def _():
        away.wait_send()

    @pl.when(x == home)
    def _():
        for k in near_first(nz):
            to_line(k).wait_send()

    own_z.wait()
    for copy in z_in:
        copy.wait_recv()
    resid = resid[0:PAD]
    for t in range(nz):
        resid = resid + z_recv[t].astype(F32)
    out[...] = resid[0:b].astype(BF16)
    for copy in pending:
        copy.wait_send()


def layer(d, args):
    def vmem(*shape, dtype=BF16):
        return pltpu.VMEM(shape, dtype)

    line = d.nz * d.b
    dma = pltpu.SemaphoreType.DMA
    inside = pl.BlockSpec(memory_space=pltpu.VMEM)
    outside = pl.BlockSpec(memory_space=pltpu.HBM)
    return pl.pallas_call(
        functools.partial(kernel, d),
        out_shape=(
            jax.ShapeDtypeStruct((d.b, d.xs), BF16),
            jax.ShapeDtypeStruct((line, d.xs), BF16),
            jax.ShapeDtypeStruct((8, d.nt), F32),
            jax.ShapeDtypeStruct((1,), jnp.int32),
        ),
        in_specs=[outside] * 14,
        out_specs=(inside, outside, inside, pl.BlockSpec(memory_space=pltpu.SMEM)),
        scratch_shapes=[
            vmem(d.b, d.width), vmem(1, d.width, dtype=F32), vmem(d.rp, d.ql), vmem(d.rp, d.ql),
            vmem(1, d.width, dtype=F32),
            pltpu.SMEM((d.b,), jnp.int32), pltpu.SMEM((d.ql // d.hd,), F32),
            pltpu.SMEM((2, d.b), jnp.int32), pltpu.SMEM((2, d.b), F32),
            vmem(d.b, d.cache, d.hd), vmem(d.b, d.cache, d.hd),
            vmem(d.width, d.ff), vmem(d.width, d.ff), vmem(d.ff, d.width),
            dma((23,)),
            vmem(d.nz, PAD, d.zb), vmem(d.nz, PAD, d.zb),
            vmem(d.nz * d.nc, PAD, d.zb // d.nc), vmem(d.nz * d.nc, PAD, d.zb // d.nc),
            vmem(d.ny * d.rp, d.ql), vmem(d.zb, d.ql),
            vmem(d.nz * d.nc, PAD, d.ql), vmem(d.nz * d.nc, PAD, d.ql),
            vmem(PAD, d.ql), vmem(d.nz, PAD, d.ql),
            vmem(line, d.zb), vmem(d.nx, line, d.zb), vmem(line, d.zb),
            vmem(line, d.xs), vmem(SLOTS, d.xs), vmem(d.ny * SLOTS, d.xs),
            vmem(d.nc, SLOTS, d.xs), vmem(d.nx, d.nc * SLOTS, d.xs),
            vmem(d.nx, d.nc * SLOTS, d.xs), vmem(d.nx, d.nc * SLOTS, d.xs),
            vmem(d.ny, SLOTS, d.xs), vmem(d.ny, SLOTS, d.xs),
            vmem(d.nz, PAD, d.xs), vmem(d.nz, PAD, d.xs),
            vmem(8, d.nt, dtype=F32), vmem(d.nz, 8, d.nt, dtype=F32),
            vmem(8, d.nt, dtype=F32), vmem(d.ny, 8, d.nt, dtype=F32),
            vmem(8, d.nt, dtype=F32), vmem(8, d.nt, dtype=F32),
            dma((9 * d.nz,)), dma((9 * d.nz,)),
            dma((5 * d.ny,)), dma((5 * d.ny,)),
            dma((1 + 2 * d.nx * d.nc,)), dma((d.nx + 2 * d.nx * d.nc,)),
            dma((d.ny + 1,)), dma((d.ny + 1,)),
        ],
        compiler_params=pltpu.CompilerParams(
            collective_id=0, has_side_effects=True, vmem_limit_bytes=60 * 1024 * 1024),
    )(*args)


def crowded(d, line, info, expert_gain, gate_weight, up_weight, down_weight):
    places = ("c", "y")
    copies = jnp.broadcast_to(line, (d.nc * d.ny, *line.shape))
    lines = lax.all_to_all(copies, places, split_axis=0, concat_axis=0, tiled=True)
    rows = lines.reshape(d.nt, d.xs)
    copies = jnp.broadcast_to(rows, (d.nx, *rows.shape))
    spans = lax.all_to_all(copies, "x", split_axis=0, concat_axis=0, tiled=True)
    full = jnp.moveaxis(spans, 0, 1).reshape(d.nt, d.width)
    wide = full.astype(F32)
    scale = lax.rsqrt(jnp.mean(wide * wide, axis=-1, keepdims=True) + 1e-06)
    normed = (wide * scale * expert_gain).astype(BF16)
    gated = jnp.dot(normed, gate_weight, preferred_element_type=F32)
    upward = jnp.dot(normed, up_weight, preferred_element_type=F32)
    hidden = (jax.nn.silu(gated) * upward).astype(BF16)
    term = jnp.dot(hidden, down_weight, preferred_element_type=F32).astype(BF16)
    tiles = jnp.moveaxis(term.reshape(d.nt, d.nx, d.xs), 1, 0)
    terms = lax.all_to_all(tiles, "x", split_axis=0, concat_axis=0, tiled=True)
    answer = terms.astype(F32).sum(axis=0).astype(BF16).astype(F32)
    mine = lax.axis_index(EP).astype(F32)
    route = jnp.where(info[0] == mine, info[2], 0.0) + jnp.where(info[1] == mine, info[3], 0.0)
    answer = answer * route[:, None]
    answer = answer.reshape(d.nc, d.ny, d.nz, d.b, d.xs).transpose(2, 1, 0, 3, 4)
    answer = answer.reshape(-1, d.b, d.xs)
    back = lax.all_to_all(answer, EP, split_axis=0, concat_axis=0, tiled=True)
    z, y, c = (lax.axis_index(name) for name in EP)
    first = ((c * d.ny + y) * d.nz + z) * d.b
    resid = lax.dynamic_slice_in_dim(rows, first, d.b, 0)
    return (resid.astype(F32) + back.sum(axis=0)).astype(BF16)


def local(
    tokens,
    mixer_gain,
    query_weight,
    key_cache,
    value_cache,
    seq_lengths,
    head_offset,
    output_weight,
    expert_gain,
    expert_ids,
    route_weight,
    gate_weight,
    up_weight,
    down_weight,
):
    nz, ny, nc, nx = (lax.axis_size(name) for name in ("z", "y", "c", "x"))
    batch, width = tokens.shape
    d = SimpleNamespace(
        nz=nz, ny=ny, nc=nc, nx=nx, b=batch, width=width, zb=width // nz, xs=width // nx,
        nb=nz // nx, rp=query_weight.shape[0], ql=query_weight.shape[1], hd=key_cache.shape[3],
        cache=key_cache.shape[1], ff=gate_weight.shape[2], nt=nz * ny * nc * batch,
        experts=nz * ny * nc,
    )
    done, line, info, most = layer(d, (
        tokens,
        mixer_gain.reshape(1, width),
        query_weight,
        key_cache.reshape(batch, d.cache, d.hd),
        value_cache.reshape(batch, d.cache, d.hd),
        seq_lengths,
        head_offset,
        output_weight.T,
        expert_gain.reshape(1, width),
        expert_ids.T,
        route_weight.T,
        gate_weight[0],
        up_weight[0],
        down_weight[0],
    ))
    return lax.cond(
        most[0] > 0,
        lambda: crowded(d, line, info, expert_gain, gate_weight[0], up_weight[0], down_weight[0]),
        lambda: done,
    )


def solution(mesh):
    split = Mesh(mesh.devices.reshape(8, 8, 2, mesh.shape["tp"]), ("z", "y", "c", "x"))
    return sharded(split)


def sharded(split):
    in_specs = (
        P(EP, None),
        P(),
        P(EP, "x"),
        P(EP, None, "x", None),
        P(EP, None, "x", None),
        P(EP),
        P("x"),
        P("x", EP),
        P(),
        P(EP, None),
        P(EP, None),
        P(EP, None, "x"),
        P(EP, None, "x"),
        P(EP, "x", None),
    )
    return jax.shard_map(local, mesh=split, in_specs=in_specs, out_specs=P(EP, "x"), check_vma=False)
```

```python
import functools
from types import SimpleNamespace

import jax
import jax.numpy as jnp
from jax import lax
from jax.experimental import pallas as pl
from jax.experimental.pallas import tpu as pltpu
from jax.sharding import Mesh
from jax.sharding import PartitionSpec as P

EP = ("z", "y", "c")
SLOTS = 16
PAD = 4
F32 = jnp.float32
BF16 = jnp.bfloat16


def iota(shape, dim):
    return lax.broadcasted_iota(jnp.int32, shape, dim)


def dot(a, b, dims=((1,), (0,)), precision=None):
    return lax.dot_general(a, b, (dims, ((), ())), precision=precision, preferred_element_type=F32)


def onehot(condition):
    return jnp.where(condition, 1.0, 0.0).astype(BF16)


def near_first(count):
    return sorted(range(1, count), key=lambda k: min(k, count - k))


def far_first(count):
    return near_first(count)[::-1]


def stacked(ref, count):
    return jnp.concatenate([ref[t].astype(F32) for t in range(count)], axis=0).astype(BF16)


def turned(value):
    return jnp.concatenate([value[:, 64:], value[:, :64]], axis=1)


def side_by_side(d, upper, lower):
    low = iota((upper.shape[0], 128), 1) < 64
    result = []
    for t in range(d.nx):
        span = slice(t // 2 * 128, t // 2 * 128 + 128)
        left, right = upper[:, span], lower[:, span]
        pair = (left, turned(right)) if t % 2 == 0 else (turned(left), right)
        result.append(jnp.where(low, *pair).astype(BF16))
    return result


def remote(src, dst, send_sem, recv_sem, **where):
    return pltpu.make_async_remote_copy(
        src_ref=src,
        dst_ref=dst,
        send_sem=send_sem,
        recv_sem=recv_sem,
        device_id=where,
        device_id_type=pl.DeviceIdType.MESH,
    )


def attention(d, q, kbuf, vbuf, lens, hoff):
    heads = d.ql // d.hd
    rows = heads * 8
    queries = jnp.concatenate([q[:, h * d.hd : (h + 1) * d.hd] for h in range(heads)], axis=0)
    queries = queries.astype(BF16)
    row = iota((rows, 1), 0)
    seq = row & 7
    head = row >> 3
    score = jnp.zeros((rows, d.cache), F32)
    length = jnp.zeros((rows, 1), jnp.int32)
    offset = jnp.zeros((rows, 1), F32)
    for b in range(d.b):
        one = dot(queries, kbuf[b], ((1,), (1,)))
        score = jnp.where(seq == b, one, score)
        length = jnp.where(seq == b, lens[b], length)
    for h in range(heads):
        offset = jnp.where(head == h, hoff[h], offset)
    score = score * (d.hd**-0.5) + offset
    valid = iota((rows, d.cache), 1) < length
    soft = jnp.log1p(jnp.exp(-jnp.abs(score)))
    log_take = jnp.minimum(score, 0.0) - soft
    log_pass = jnp.where(valid, jnp.minimum(-score, 0.0) - soft, 0.0)
    blocks = d.cache // 128
    pieces = [log_pass[:, i * 128 : (i + 1) * 128] for i in range(blocks)]
    after = (iota((128, 128), 0) > iota((128, 128), 1)).astype(F32)
    inside = dot(jnp.concatenate(pieces, axis=0), after, precision=lax.Precision.HIGHEST)
    later = jnp.zeros((rows, 1), F32)
    sums = [None] * blocks
    for i in range(blocks - 1, -1, -1):
        sums[i] = inside[i * rows : (i + 1) * rows] + later
        later = later + jnp.sum(pieces[i], axis=1, keepdims=True)
    weight = jnp.where(valid, jnp.exp(log_take + jnp.concatenate(sums, axis=1)), 0.0).astype(BF16)
    total = jnp.zeros((rows, d.hd), F32)
    for b in range(d.b):
        total = jnp.where(seq == b, dot(weight, vbuf[b]), total)
    return jnp.concatenate([total[h * 8 : (h + 1) * 8] for h in range(heads)], axis=1).astype(BF16)


def kernel(d, *refs):
    (tokens_in, mgain_in, wq_in_hbm, key, val, lens_in, hoff_in, wo_in_hbm, egain_in, ids_in, rw_in,
     gate, up, down) = refs[:14]
    out, line_out, info_out, most_out = refs[14:18]
    (tokens, mgain, wq, wo, egain, lens, hoff, ids, rw,
     kbuf, vbuf, gbuf, ubuf, dbuf, load_sem,
     ta_send, ta_recv, qa_send, qa_recv, wq_all, wo_all, qp_send, qp_recv, mx_send, mx_recv,
     tk_all, tk_recv, f_send, f_recv, gains,
     pt_send, pt_recv, rb_send, line_rows, own_send, rows, s_send, s_recv, h_send, h_recv,
     y_send, y_recv,
     info_a, info_az, info_b, info_by, info_c, info_cc,
     zs, zr, ys, yr, xs, xr, cs, cr, fs, fr, gs, gr) = refs[18:]
    z, y, c, x = (lax.axis_index(name) for name in ("z", "y", "c", "x"))
    nz, ny, nc, nx, b = d.nz, d.ny, d.nc, d.nx, d.b
    other = 1 - c
    slot = c * ny + y
    line = nz * b
    home = z // d.nb
    MESH = pl.DeviceIdType.MESH

    def up_z(k):
        return lax.rem(z + k, nz)

    def up_y(k):
        return lax.rem(y + k, ny)

    def up_x(k):
        return lax.rem(x + k, nx)

    def up_c(k):
        return lax.rem(c + k, nc)

    barrier = pltpu.get_barrier_semaphore()
    peers = [{"z": up_z(k), "c": up_c(j)} for k in far_first(nz) for j in range(nc)]
    peers += [{"y": up_y(k)} for k in far_first(ny)]
    peers += [{"x": up_x(k), "c": up_c(j)} for k in far_first(nx) for j in range(nc)]
    peers += [{"c": other}]
    for peer in peers:
        pl.semaphore_signal(barrier, inc=1, device_id=peer, device_id_type=MESH)

    small = [
        pltpu.make_async_copy(src, dst, load_sem.at[14 + i])
        for i, (src, dst) in enumerate([
            (tokens_in, tokens), (mgain_in, mgain), (wq_in_hbm, wq), (ids_in, ids), (rw_in, rw),
            (wo_in_hbm, wo), (lens_in, lens), (hoff_in, hoff), (egain_in, egain),
        ])
    ]
    for copy in small:
        copy.start()
    loads = [(key, kbuf), (val, vbuf), (down, dbuf)]
    for t in range(nx):
        loads += [(gate.at[:, t], gbuf.at[t]), (up.at[:, t], ubuf.at[t])]
    loads = [
        pltpu.make_async_copy(src, dst, load_sem.at[23 + i]) for i, (src, dst) in enumerate(loads)
    ]
    for copy in loads:
        copy.start()
    small[2].wait()
    pl.semaphore_wait(barrier, len(peers))
    pending = []

    def send(copy):
        copy.start()
        pending.append(copy)
        return copy

    def keep(number, src, dst):
        copy = pltpu.make_async_copy(src, dst, load_sem.at[number])
        copy.start()
        return copy

    own_rows = pl.multiple_of(y * d.rp, 8)
    own_piece = pl.multiple_of((y * nc + c) * d.rp, 8)
    wq_in = [
        send(remote(wq, wq_all.at[pl.ds(own_rows, d.rp)], ys.at[k], yr.at[k], y=up_y(k)))
        for k in far_first(ny)
    ]
    own_q = keep(5, wq, wq_all.at[pl.ds(own_rows, d.rp)])
    for copy in small[:2] + small[3:]:
        copy.wait()

    wide = tokens[...].astype(F32)
    scale = lax.rsqrt(jnp.mean(wide * wide, axis=1, keepdims=True) + 1e-06)
    normed = (wide * scale * mgain[...]).astype(BF16).astype(F32)
    filler = jnp.zeros((PAD - b, d.width), F32)
    normed = jnp.concatenate([normed, filler], axis=0)
    plain = jnp.concatenate([wide, filler], axis=0).astype(BF16)
    for t in range(nz):
        ta_send[t] = plain[:, t * d.zb : (t + 1) * d.zb]
    share = ny * d.rp
    depth, tall = d.rp.bit_length() - 1, share.bit_length() - 1
    to = iota((d.zb, d.zb), 1)
    source = ((((to & (share - 1)) >> depth) * nc + (to >> tall)) << depth) + (to & (d.rp - 1))
    order = onehot(iota((d.zb, d.zb), 0) == source)
    moved = dot(
        jnp.concatenate([normed[:, t * d.zb : (t + 1) * d.zb] for t in range(nz)], axis=0).astype(BF16),
        order).astype(BF16)
    for t in range(nz):
        for j in range(nc):
            qa_send[t * nc + j] = moved[t * PAD : (t + 1) * PAD, j * share : (j + 1) * share]
    lane = iota((8, d.nt), 1)
    field = iota((8, d.nt), 0)
    info = jnp.zeros((8, d.nt), F32)
    for r in range(b):
        here = lane == slot * line + z * b + r
        for j, number in enumerate((
            ids[0, r].astype(F32), ids[1, r].astype(F32), rw[0, r], rw[1, r],
        )):
            info = jnp.where(here & (field == j), number, info)
    info_a[...] = info
    zc = [(k, j) for k in far_first(nz) for j in range(nc)] + [(0, j) for j in range(1, nc)]
    me = z * nc + c

    def there(k, j):
        return up_z(k) * nc + up_c(j)

    def zc_exchange(base, source, everything):
        return [
            send(remote(
                source.at[there(k, j)], everything.at[me],
                zs.at[base + k * nc + j], zr.at[base + k * nc + j], z=up_z(k), c=up_c(j)))
            for k, j in zc
        ]

    def from_y(k):
        return lax.rem(y - k + ny, ny)

    qa_in = zc_exchange(0, qa_send, qa_recv)
    own_a = keep(7, qa_send.at[me], qa_recv.at[me])
    info_in = [
        send(remote(info_a, info_az.at[z], zs.at[4 * nz + k], zr.at[4 * nz + k], z=up_z(k)))
        for k in far_first(nz)
    ]
    wo_in = {
        k: send(remote(wo, wo_all.at[pl.ds(own_piece, d.rp)], ys.at[ny + k], yr.at[ny + k], y=up_y(k)))
        for k in far_first(ny)
    }
    own_o = keep(6, wo, wo_all.at[pl.ds(own_piece, d.rp)])
    wo_fwd = [send(remote(wo, wo_all.at[pl.ds(own_piece, d.rp)], cs.at[0], cr.at[0], c=other))]
    ta_in = [
        send(remote(ta_send.at[up_z(k)], ta_recv.at[z], zs.at[5 * nz + k], zr.at[5 * nz + k], z=up_z(k)))
        for k in far_first(nz)
    ]
    own_t = keep(8, ta_send.at[z], ta_recv.at[z])

    for copy in qa_in:
        copy.wait_recv()
    own_a.wait()
    own_q.wait()
    rows_a = stacked(qa_recv, nz * nc)
    for copy in wq_in:
        copy.wait_recv()
    partial = dot(rows_a, wq_all[...]).astype(BF16)
    for t in range(nz * nc):
        qp_send[t] = partial[t * PAD : (t + 1) * PAD]
    qp_in = zc_exchange(2 * nz, qp_send, qp_recv)
    own_p = keep(9, qp_send.at[me], qp_recv.at[me])

    for k in near_first(ny):
        wo_in[k].wait_recv()
        part = wo_all.at[pl.ds(pl.multiple_of((from_y(k) * nc + c) * d.rp, 8), d.rp)]
        wo_fwd.append(send(remote(part, part, cs.at[k], cr.at[k], c=other)))
    for copy in info_in:
        copy.wait_recv()
    info = info_a[...]
    for k in range(1, nz):
        info = info + info_az[up_z(k)]
    info_b[...] = info
    info_y_in = [
        send(remote(info_b, info_by.at[y], ys.at[2 * ny + k], yr.at[2 * ny + k], y=up_y(k)))
        for k in far_first(ny)
    ]
    loads[0].wait()
    loads[1].wait()

    for copy in qp_in:
        copy.wait_recv()
    own_p.wait()
    q = qp_recv[0].astype(F32)
    for t in range(1, nz * nc):
        q = q + qp_recv[t].astype(F32)
    q = jnp.concatenate([q, jnp.zeros((8 - PAD, d.ql), F32)], axis=0)
    mixed = attention(d, q, kbuf, vbuf, lens, hoff)
    mx_send[...] = mixed[0:PAD]
    mx_in = [
        send(remote(mx_send, mx_recv.at[z], zs.at[6 * nz + k], zr.at[6 * nz + k], z=up_z(k)))
        for k in far_first(nz)
    ]
    own_m = keep(10, mx_send, mx_recv.at[z])

    for copy in info_y_in:
        copy.wait_recv()
    info = info_b[...]
    for k in range(1, ny):
        info = info + info_by[up_y(k)]
    info_c[...] = info
    info_c_in = send(remote(info_c, info_cc, cs.at[ny], cr.at[ny], c=other))

    pick_t = iota((line, nz * PAD), 0)
    pick_s = iota((line, nz * PAD), 1)
    within = pick_s & (PAD - 1)
    pick = onehot((within < b) & ((pick_s >> (PAD.bit_length() - 1)) * b + within == pick_t))
    for copy in ta_in:
        copy.wait_recv()
    own_t.wait()
    tok = dot(pick, stacked(ta_recv, nz))
    own_token = onehot(iota((d.nt, line), 0) == iota((d.nt, line), 1) + slot * line)
    count = float(ny * nc)
    own_ids = dot(info_b[...].astype(BF16), own_token)[0:1]
    zone = iota((8, line), 0).astype(F32) * count
    bound = onehot((own_ids >= zone) & (own_ids < zone + count))
    bound_rank = dot(bound, onehot(iota((line, line), 0) < iota((line, line), 1)))
    wide_rows = nz * SLOTS // 2
    widen = onehot((iota((wide_rows, 8), 0) >> 3) == iota((wide_rows, 8), 1))
    bound = dot(widen, bound) > 0.5
    bound_rank = dot(widen, bound_rank.astype(BF16))
    number = (iota((wide_rows, line), 0) & 7).astype(F32)
    pack_all = jnp.concatenate(
        [onehot(bound & (bound_rank == number)), onehot(bound & (bound_rank == number + 8.0))], axis=0)
    moved = dot(pack_all, tok.astype(BF16))
    for t, part in enumerate(side_by_side(d, moved[:wide_rows], moved[wide_rows:])):
        tk_all[t] = part.reshape(nz, SLOTS // 2, 128)
    tk_in = [
        send(remote(tk_all.at[x, up_z(k)], tk_recv.at[z], zs.at[9 * nz + k], zr.at[9 * nz + k], z=up_z(k)))
        for k in far_first(nz)
    ]
    own_tk = keep(0, tk_all.at[x, z], tk_recv.at[z])
    pack_all = dot(pack_all, pick).astype(BF16)
    for t in range(nx):
        gains[t] = jnp.concatenate(
            [egain[:, u * d.zb + t * 64 : u * d.zb + t * 64 + 64] for u in range(nz)], axis=1)
    for copy in wo_fwd:
        copy.wait_recv()
    own_o.wait()
    for copy in mx_in:
        copy.wait_recv()
    own_m.wait()
    all_mixed = stacked(mx_recv, nz)
    moved = dot(dot(pack_all, all_mixed).astype(BF16), wo_all[...], ((1,), (1,)))
    for t, part in enumerate(side_by_side(d, moved[:wide_rows], moved[wide_rows:])):
        f_send[t] = part.reshape(nz, SLOTS // 2, 128)
    f_in = [
        send(remote(
            f_send.at[up_x(j), up_z(k)], f_recv.at[x, z],
            fs.at[k * nx + j], fr.at[k * nx + j], x=up_x(j), z=up_z(k)))
        for k in far_first(nz) + [0] for j in far_first(nx) + [0] if k or j
    ]
    own_f = keep(1, f_send.at[x, z], f_recv.at[x, z])
    tight = dot(pick, all_mixed).astype(BF16)
    pt_send[...] = dot(tight, wo_all[...], ((1,), (1,))).astype(BF16)

    away = remote(pt_send, pt_recv.at[x], xs.at[0], xr.at[x], x=home)
    own_lanes = pl.multiple_of(lax.rem(z, d.nb) * d.zb, d.zb)
    own_block = line_rows.at[:, pl.ds(own_lanes, d.zb)]
    own_b = pltpu.make_async_copy(rb_send, own_block, load_sem.at[11])

    def to_line(k):
        return remote(
            rb_send, own_block, zs.at[7 * nz + k], zr.at[7 * nz + lax.rem(z, d.nb)], z=up_z(k))

    @pl.when(x != home)
    def _():
        away.start()

    info_c_in.wait_recv()
    info = info_c[...] + info_cc[...]
    info_out[...] = info
    id0 = info[0:1]
    id1 = info[1:2]
    low = z.astype(F32) * count
    half_width = ny * line

    def line_of(places):
        return jnp.floor((places.astype(F32) + 0.5) * (1.0 / line))

    token_line = line_of(iota((1, d.nt), 1))
    token_half = jnp.where(token_line >= ny, 1.0, 0.0)
    ours = token_half == c.astype(F32)
    staying = (id0 >= low) & (id0 < low + count)
    stay = jnp.where(staying, 1.0, 0.0)
    hits = []
    for j in range(nc):
        expert = low + (y * nc + j).astype(F32)
        hits.append((jnp.where(id0 == expert, 1.0, 0.0), jnp.where(id1 == expert, 1.0, 0.0)))
    first, second = iota((d.nt, d.nt), 0), iota((d.nt, d.nt), 1)
    earlier = first < second
    same_line = line_of(first) == line_of(second)
    same_half = (first < half_width) == (second < half_width)
    line_rank = dot(jnp.broadcast_to(stay, (8, d.nt)).astype(BF16), onehot(earlier & same_line))[0:1]
    hit_rows = jnp.concatenate([h0 + h1 for h0, h1 in hits], axis=0)
    hit_rank = dot(hit_rows.astype(BF16), onehot(earlier & same_half))
    numbers = iota((SLOTS, d.nt), 0).astype(F32)
    chosen = [
        onehot((numbers == hit_rank[j : j + 1]) & (hit_rows[j : j + 1] > 0.5) & ours) for j in range(nc)
    ]
    routes = [h0 * info[2:3] + h1 * info[3:4] for h0, h1 in hits]
    slot_route = jnp.concatenate([
        jnp.sum(chosen[j].astype(F32) * routes[j], axis=1, keepdims=True) for j in range(nc)], axis=0)
    chosen = jnp.concatenate(chosen, axis=0)
    kept = ny * SLOTS
    place = (token_line - c.astype(F32) * ny) * SLOTS + line_rank
    packed = onehot(
        (iota((kept, d.nt), 0).astype(F32) == place) & staying & ours & (line_rank < SLOTS - 0.5))
    chosen_tokens = chosen
    chosen = dot(chosen, packed, ((1,), (1,))).astype(BF16)
    owner_s = iota((ny * nz * PAD, d.nt), 0)
    owner_t = iota((ny * nz * PAD, d.nt), 1) - c * half_width
    r_of = owner_s & (PAD - 1)
    first_of = (owner_s >> (PAD.bit_length() - 1)) * b
    owners = onehot((r_of < b) & (first_of + r_of == owner_t))
    owners = dot(owners, chosen_tokens, ((1,), (1,)))
    homes = []
    for r in range(b):
        last = onehot((r_of == b) & (first_of + r == owner_t))
        last = dot(last, chosen_tokens, ((1,), (1,)))
        homes.append(jnp.concatenate([owners, last], axis=1).astype(BF16))
    expert = iota((d.experts, d.nt), 0).astype(F32)
    named = onehot((id0 == expert) | (id1 == expert))
    group_t = iota((d.nt, 128), 0)
    group_g = iota((d.nt, 128), 1)
    halves = dot(named, onehot((group_t >= half_width) == (group_g > 0)))
    zone = iota((8, d.nt), 0).astype(F32) * count
    lines = dot(onehot((id0 >= zone) & (id0 < zone + count)), onehot(line_of(group_t) == group_g.astype(F32)))
    most = jnp.maximum(jnp.max(halves), jnp.max(lines))
    most_out[0] = jnp.where(most > SLOTS, 1, 0)

    own_tk.wait()
    for copy in tk_in:
        copy.wait_recv()
    own_f.wait()
    for copy in f_in:
        copy.wait_recv()
    summed = []
    for u in range(nz):
        total = tk_recv[u].astype(F32)
        for t in range(nx):
            total = total + f_recv[t, u].astype(F32)
        summed.append(total)
    low_lanes = iota((SLOTS // 2, 128), 1) < 64
    for u in range(0, nz, 2):
        span = slice(u * 64, u * 64 + 128)
        own_send[:, span] = jnp.concatenate([
            jnp.where(low_lanes, summed[u], turned(summed[u + 1])),
            jnp.where(low_lanes, turned(summed[u]), summed[u + 1])], axis=0).astype(BF16)
    own_slots = pl.ds(pl.multiple_of(y * SLOTS, SLOTS), SLOTS)
    rows_in = [
        send(remote(own_send, rows.at[own_slots], ys.at[3 * ny + k], yr.at[3 * ny + k], y=up_y(k)))
        for k in far_first(ny)
    ]
    own_s = keep(13, own_send, rows.at[own_slots])
    @pl.when(x == home)
    def _():
        total = tok + pt_send[...].astype(F32)
        for k in range(1, nx):
            source = lax.rem(x + k, nx)
            remote(pt_send, pt_recv.at[source], xs.at[0], xr.at[source], x=source).wait_recv()
            total = total + pt_recv[source].astype(F32)
        rb_send[...] = total.astype(BF16)
        own_b.start()
        for k in far_first(nz):
            to_line(k).start()

    own_s.wait()
    for copy in rows_in:
        copy.wait_recv()

    s_send[...] = dot(chosen, rows[...]).astype(BF16).reshape(nc, SLOTS, d.xs)
    xc = [(k, j) for k in far_first(nx) for j in range(nc)] + [(0, j) for j in range(1, nc)]
    our_slots = pl.ds(pl.multiple_of(c * SLOTS, SLOTS), SLOTS)
    s_in = [
        send(remote(
            s_send.at[up_c(j)], s_recv.at[x, our_slots],
            xs.at[1 + k * nc + j], xr.at[nx + k * nc + j], x=up_x(k), c=up_c(j)))
        for k, j in xc
    ]
    own_s = keep(5, s_send.at[c], s_recv.at[x, our_slots])
    for copy in loads[2:]:
        copy.wait()
    own_s.wait()
    for copy in s_in:
        copy.wait_recv()
    wide = [s_recv[t].astype(F32) for t in range(nx)]
    square = sum(jnp.sum(part * part, axis=1, keepdims=True) for part in wide)
    scale = lax.rsqrt(square / d.width + 1e-06)
    gated = jnp.zeros((nc * SLOTS, d.ff), F32)
    upward = jnp.zeros((nc * SLOTS, d.ff), F32)
    for t in range(nx):
        part = (wide[t] * scale * gains[t]).astype(BF16)
        gated = gated + dot(part, gbuf[t].reshape(d.xs, d.ff))
        upward = upward + dot(part, ubuf[t].reshape(d.xs, d.ff))
    hidden = (gated / (1.0 + jnp.exp(-gated)) * upward).astype(BF16)
    for t in range(nx):
        h_send[t] = dot(hidden, dbuf[:, t * d.xs : (t + 1) * d.xs]).astype(BF16)

    def to_half(j):
        return pl.ds(pl.multiple_of(up_c(j) * SLOTS, SLOTS), SLOTS)

    h_in = [
        send(remote(
            h_send.at[up_x(k), to_half(j)], h_recv.at[x, our_slots],
            xs.at[1 + nx * nc + k * nc + j], xr.at[nx + nx * nc + k * nc + j], x=up_x(k), c=up_c(j)))
        for k, j in xc
    ]
    own_h = keep(6, h_send.at[x, our_slots], h_recv.at[x, our_slots])
    own_h.wait()
    for copy in h_in:
        copy.wait_recv()
    total = h_recv[0].astype(F32)
    for t in range(1, nx):
        total = total + h_recv[t].astype(F32)
    answer = total.astype(BF16).astype(F32) * slot_route
    part = d.xs // PAD
    for r in range(b):
        both = jnp.concatenate([answer[:, r * part : (r + 1) * part], answer[:, b * part :]], axis=0)
        y_send[:, :, r * part : (r + 1) * part] = (
            dot(homes[r], both.astype(BF16)).reshape(ny * nz, PAD, part).astype(BF16))

    def give(t, k):
        return remote(
            y_send.at[up_y(k) * nz + t], y_recv.at[y * nz + z],
            gs.at[t * ny + k], gr.at[z * ny + k], z=t, y=up_y(k))

    for t in range(nz):
        for k in far_first(ny):
            send(give(t, k))

        @pl.when(z != t)
        def _():
            give(t, 0).start()

    given = nz * (ny - 1)
    own_y = keep(7, y_send.at[y * nz + z], y_recv.at[y * nz + z])
    for j in range(d.nb):
        source = x * d.nb + j

        @pl.when(z != source)
        def _():
            block = line_rows.at[:, pl.ds(j * d.zb, d.zb)]
            remote(rb_send, block, zs.at[0], zr.at[7 * nz + j], z=source).wait_recv()

    @pl.when(x == home)
    def _():
        own_b.wait()

    save = keep(12, line_rows, line_out)
    mine_t = iota((8, line), 1)
    mine_r = iota((8, line), 0)
    resid = dot(onehot((mine_r < b) & (mine_t == mine_r + z * b)), line_rows[...])
    save.wait()

    @pl.when(x != home)
    def _():
        away.wait_send()

    @pl.when(x == home)
    def _():
        for k in near_first(nz):
            to_line(k).wait_send()

    for copy in pending[:-given]:
        copy.wait_send()
    own_y.wait()
    for t in range(nz):
        for k in near_first(ny):
            remote(
                y_send.at[0], y_recv.at[from_y(k) * nz + t], gs.at[0], gr.at[t * ny + k],
                z=t, y=from_y(k)).wait_recv()

        @pl.when(z != t)
        def _():
            remote(
                y_send.at[0], y_recv.at[y * nz + t], gs.at[0], gr.at[t * ny], z=t).wait_recv()

    total = y_recv[0].astype(F32)
    for t in range(1, ny * nz):
        total = total + y_recv[t].astype(F32)
    last = jnp.concatenate([total[b : b + 1, r * part : (r + 1) * part] for r in range(b)], axis=0)
    out[...] = (resid[0:b] + jnp.concatenate([total[0:b], last], axis=1)).astype(BF16)
    for t in range(nz):
        @pl.when(z != t)
        def _():
            give(t, 0).wait_send()

    for copy in pending[-given:]:
        copy.wait_send()


def layer(d, args):
    def vmem(*shape, dtype=BF16):
        return pltpu.VMEM(shape, dtype)

    line = d.nz * d.b
    dma = pltpu.SemaphoreType.DMA
    inside = pl.BlockSpec(memory_space=pltpu.VMEM)
    outside = pl.BlockSpec(memory_space=pltpu.HBM)
    return pl.pallas_call(
        functools.partial(kernel, d),
        out_shape=(
            pltpu.VMEM((d.b, d.xs), BF16),
            jax.ShapeDtypeStruct((line, d.xs), BF16),
            jax.ShapeDtypeStruct((8, d.nt), F32),
            jax.ShapeDtypeStruct((1,), jnp.int32),
        ),
        in_specs=[outside] * 14,
        out_specs=(inside, outside, inside, pl.BlockSpec(memory_space=pltpu.SMEM)),
        scratch_shapes=[
            vmem(d.b, d.width), vmem(1, d.width, dtype=F32), vmem(d.rp, d.ql), vmem(d.rp, d.ql),
            vmem(1, d.width, dtype=F32),
            pltpu.SMEM((d.b,), jnp.int32), pltpu.SMEM((d.ql // d.hd,), F32),
            pltpu.SMEM((2, d.b), jnp.int32), pltpu.SMEM((2, d.b), F32),
            vmem(d.b, d.cache, d.hd), vmem(d.b, d.cache, d.hd),
            vmem(d.nx, d.nz, d.zb // d.nx, d.ff), vmem(d.nx, d.nz, d.zb // d.nx, d.ff), vmem(d.ff, d.width),
            dma((26 + 2 * d.nx,)),
            vmem(d.nz, PAD, d.zb), vmem(d.nz, PAD, d.zb),
            vmem(d.nz * d.nc, PAD, d.zb // d.nc), vmem(d.nz * d.nc, PAD, d.zb // d.nc),
            vmem(d.ny * d.rp, d.ql), vmem(d.zb, d.ql),
            vmem(d.nz * d.nc, PAD, d.ql), vmem(d.nz * d.nc, PAD, d.ql),
            vmem(PAD, d.ql), vmem(d.nz, PAD, d.ql),
            vmem(d.nx, d.nz, SLOTS // 2, 128), vmem(d.nz, SLOTS // 2, 128),
            vmem(d.nx, d.nz, SLOTS // 2, 128), vmem(d.nx, d.nz, SLOTS // 2, 128),
            vmem(d.nx, 1, d.xs, dtype=F32),
            vmem(line, d.zb), vmem(d.nx, line, d.zb), vmem(line, d.zb),
            vmem(line, d.xs), vmem(SLOTS, d.xs), vmem(d.ny * SLOTS, d.xs),
            vmem(d.nc, SLOTS, d.xs), vmem(d.nx, d.nc * SLOTS, d.xs),
            vmem(d.nx, d.nc * SLOTS, d.xs), vmem(d.nx, d.nc * SLOTS, d.xs),
            vmem(d.ny * d.nz, PAD, d.xs // PAD * d.b), vmem(d.ny * d.nz, PAD, d.xs // PAD * d.b),
            vmem(8, d.nt, dtype=F32), vmem(d.nz, 8, d.nt, dtype=F32),
            vmem(8, d.nt, dtype=F32), vmem(d.ny, 8, d.nt, dtype=F32),
            vmem(8, d.nt, dtype=F32), vmem(8, d.nt, dtype=F32),
            dma((10 * d.nz,)), dma((10 * d.nz,)),
            dma((5 * d.ny,)), dma((5 * d.ny,)),
            dma((1 + 2 * d.nx * d.nc,)), dma((d.nx + 2 * d.nx * d.nc,)),
            dma((d.ny + 1,)), dma((d.ny + 1,)),
            dma((d.nz * d.nx,)), dma((d.nz * d.nx,)),
            dma((d.nz * d.ny,)), dma((d.nz * d.ny,)),
        ],
        compiler_params=pltpu.CompilerParams(
            collective_id=0, has_side_effects=True, vmem_limit_bytes=60 * 1024 * 1024),
    )(*args)


def crowded(d, line, info, expert_gain, gate_weight, up_weight, down_weight):
    places = ("c", "y")
    copies = jnp.broadcast_to(line, (d.nc * d.ny, *line.shape))
    lines = lax.all_to_all(copies, places, split_axis=0, concat_axis=0, tiled=True)
    rows = lines.reshape(d.nt, d.xs)
    copies = jnp.broadcast_to(rows, (d.nx, *rows.shape))
    spans = lax.all_to_all(copies, "x", split_axis=0, concat_axis=0, tiled=True)
    full = jnp.moveaxis(spans, 0, 1).reshape(d.nt, d.width)
    wide = full.astype(F32)
    scale = lax.rsqrt(jnp.mean(wide * wide, axis=-1, keepdims=True) + 1e-06)
    normed = (wide * scale * expert_gain).astype(BF16)
    gated = jnp.dot(normed, gate_weight, preferred_element_type=F32)
    upward = jnp.dot(normed, up_weight, preferred_element_type=F32)
    hidden = (jax.nn.silu(gated) * upward).astype(BF16)
    term = jnp.dot(hidden, down_weight, preferred_element_type=F32).astype(BF16)
    tiles = jnp.moveaxis(term.reshape(d.nt, d.nx, d.xs), 1, 0)
    terms = lax.all_to_all(tiles, "x", split_axis=0, concat_axis=0, tiled=True)
    answer = terms.astype(F32).sum(axis=0).astype(BF16).astype(F32)
    mine = lax.axis_index(EP).astype(F32)
    route = jnp.where(info[0] == mine, info[2], 0.0) + jnp.where(info[1] == mine, info[3], 0.0)
    answer = answer * route[:, None]
    answer = answer.reshape(d.nc, d.ny, d.nz, d.b, d.xs).transpose(2, 1, 0, 3, 4)
    answer = answer.reshape(-1, d.b, d.xs)
    back = lax.all_to_all(answer, EP, split_axis=0, concat_axis=0, tiled=True)
    z, y, c = (lax.axis_index(name) for name in EP)
    first = ((c * d.ny + y) * d.nz + z) * d.b
    resid = lax.dynamic_slice_in_dim(rows, first, d.b, 0)
    return (resid.astype(F32) + back.sum(axis=0)).astype(BF16)


def local(
    tokens,
    mixer_gain,
    query_weight,
    key_cache,
    value_cache,
    seq_lengths,
    head_offset,
    output_weight,
    expert_gain,
    expert_ids,
    route_weight,
    gate_weight,
    up_weight,
    down_weight,
):
    nz, ny, nc, nx = (lax.axis_size(name) for name in ("z", "y", "c", "x"))
    batch, width = tokens.shape
    d = SimpleNamespace(
        nz=nz, ny=ny, nc=nc, nx=nx, b=batch, width=width, zb=width // nz, xs=width // nx,
        nb=nz // nx, rp=query_weight.shape[0], ql=query_weight.shape[1], hd=key_cache.shape[3],
        cache=key_cache.shape[1], ff=gate_weight.shape[2], nt=nz * ny * nc * batch,
        experts=nz * ny * nc,
    )
    done, line, info, most = layer(d, (
        tokens,
        mixer_gain.reshape(1, width),
        query_weight,
        key_cache.reshape(batch, d.cache, d.hd),
        value_cache.reshape(batch, d.cache, d.hd),
        seq_lengths,
        head_offset,
        output_weight.T,
        expert_gain.reshape(1, width),
        expert_ids.T,
        route_weight.T,
        gate_weight.reshape(nz, nx, d.zb // nx, d.ff),
        up_weight.reshape(nz, nx, d.zb // nx, d.ff),
        down_weight[0],
    ))
    return lax.cond(
        most[0] > 0,
        lambda: crowded(d, line, info, expert_gain, gate_weight[0], up_weight[0], down_weight[0]),
        lambda: done,
    )


def solution(mesh):
    split = Mesh(mesh.devices.reshape(8, 8, 2, mesh.shape["tp"]), ("z", "y", "c", "x"))
    return sharded(split)


def sharded(split):
    in_specs = (
        P(EP, None),
        P(),
        P(EP, "x"),
        P(EP, None, "x", None),
        P(EP, None, "x", None),
        P(EP),
        P("x"),
        P("x", EP),
        P(),
        P(EP, None),
        P(EP, None),
        P(EP, None, "x"),
        P(EP, None, "x"),
        P(EP, "x", None),
    )
    return jax.shard_map(local, mesh=split, in_specs=in_specs, out_specs=P(EP, "x"), check_vma=False)
```

```python
import functools
from types import SimpleNamespace

import jax
import jax.numpy as jnp
from jax import lax
from jax.experimental import pallas as pl
from jax.experimental.pallas import tpu as pltpu
from jax.sharding import Mesh
from jax.sharding import PartitionSpec as P

EP = ("z", "y", "c")
SLOTS = 16
PAD = 4
F32 = jnp.float32
BF16 = jnp.bfloat16


def iota(shape, dim):
    return lax.broadcasted_iota(jnp.int32, shape, dim)


def dot(a, b, dims=((1,), (0,)), precision=None):
    return lax.dot_general(a, b, (dims, ((), ())), precision=precision, preferred_element_type=F32)


def onehot(condition):
    return jnp.where(condition, 1.0, 0.0).astype(BF16)


def near_first(count):
    return sorted(range(1, count), key=lambda k: min(k, count - k))


def far_first(count):
    return near_first(count)[::-1]


def stacked(ref, count):
    return jnp.concatenate([ref[t].astype(F32) for t in range(count)], axis=0).astype(BF16)


def turned(value):
    return jnp.concatenate([value[:, 64:], value[:, :64]], axis=1)


def side_by_side(d, upper, lower):
    low = iota((upper.shape[0], 128), 1) < 64
    result = []
    for t in range(d.nx):
        span = slice(t // 2 * 128, t // 2 * 128 + 128)
        left, right = upper[:, span], lower[:, span]
        pair = (left, turned(right)) if t % 2 == 0 else (turned(left), right)
        result.append(jnp.where(low, *pair).astype(BF16))
    return result


def remote(src, dst, send_sem, recv_sem, **where):
    return pltpu.make_async_remote_copy(
        src_ref=src,
        dst_ref=dst,
        send_sem=send_sem,
        recv_sem=recv_sem,
        device_id=where,
        device_id_type=pl.DeviceIdType.MESH,
    )


def attention(d, q, kbuf, vbuf, lens, hoff):
    heads = d.ql // d.hd
    rows = heads * PAD
    queries = jnp.concatenate([q[:, h * d.hd : (h + 1) * d.hd] for h in range(heads)], axis=0)
    queries = queries.astype(BF16)
    row = iota((rows, 1), 0)
    seq = row & (PAD - 1)
    head = row >> (PAD.bit_length() - 1)
    score = jnp.zeros((rows, d.cache), F32)
    length = jnp.zeros((rows, 1), jnp.int32)
    offset = jnp.zeros((rows, 1), F32)
    for b in range(d.b):
        one = dot(queries, kbuf[b], ((1,), (1,)))
        score = jnp.where(seq == b, one, score)
        length = jnp.where(seq == b, lens[b], length)
    for h in range(heads):
        offset = jnp.where(head == h, hoff[h], offset)
    score = score * (d.hd**-0.5) + offset
    valid = iota((rows, d.cache), 1) < length
    soft = jnp.log1p(jnp.exp(-jnp.abs(score)))
    log_take = jnp.minimum(score, 0.0) - soft
    log_pass = jnp.where(valid, jnp.minimum(-score, 0.0) - soft, 0.0)
    blocks = d.cache // 128
    pieces = [log_pass[:, i * 128 : (i + 1) * 128] for i in range(blocks)]
    after = (iota((128, 128), 0) > iota((128, 128), 1)).astype(F32)
    inside = dot(jnp.concatenate(pieces, axis=0), after, precision=lax.Precision.HIGHEST)
    later = jnp.zeros((rows, 1), F32)
    sums = [None] * blocks
    for i in range(blocks - 1, -1, -1):
        sums[i] = inside[i * rows : (i + 1) * rows] + later
        later = later + jnp.sum(pieces[i], axis=1, keepdims=True)
    weight = jnp.where(valid, jnp.exp(log_take + jnp.concatenate(sums, axis=1)), 0.0).astype(BF16)
    total = jnp.zeros((rows, d.hd), F32)
    for b in range(d.b):
        total = jnp.where(seq == b, dot(weight, vbuf[b]), total)
    return jnp.concatenate([total[h * PAD : (h + 1) * PAD] for h in range(heads)], axis=1).astype(BF16)


def kernel(d, *refs):
    (tokens_in, mgain_in, wq_in_hbm, key, val, lens_in, hoff_in, wo_in_hbm, egain_in, ids_in, rw_in,
     gate, up, down) = refs[:14]
    out, line_out, info_out, most_out = refs[14:18]
    (tokens, mgain, wq, wo, egain, lens, hoff, ids, rw,
     kbuf, vbuf, gbuf, ubuf, dbuf, load_sem,
     ta_send, ta_recv, qa_send, qa_recv, wq_all, wo_all, qp_send, qp_recv, mx_send, mx_recv,
     tk_all, tk_recv, f_send, f_recv, gains,
     pt_send, pt_recv, rb_send, line_rows, own_send, rows, s_send, s_recv, h_send, h_recv,
     y_send, y_recv,
     info_a, info_az, info_b, info_by, info_cc,
     zs, zr, ys, yr, xs, xr, cs, cr, fs, fr, gs, gr) = refs[18:]
    z, y, c, x = (lax.axis_index(name) for name in ("z", "y", "c", "x"))
    nz, ny, nc, nx, b = d.nz, d.ny, d.nc, d.nx, d.b
    other = 1 - c
    slot = c * ny + y
    line = nz * b
    home = z // d.nb
    MESH = pl.DeviceIdType.MESH

    def up_z(k):
        return lax.rem(z + k, nz)

    def up_y(k):
        return lax.rem(y + k, ny)

    def up_x(k):
        return lax.rem(x + k, nx)

    def up_c(k):
        return lax.rem(c + k, nc)

    barrier = pltpu.get_barrier_semaphore()
    peers = [{"z": up_z(k), "c": up_c(j)} for k in far_first(nz) for j in range(nc)]
    peers += [{"y": up_y(k)} for k in far_first(ny)]
    peers += [{"x": up_x(k), "c": up_c(j)} for k in far_first(nx) for j in range(nc)]
    peers += [{"c": other}]
    for peer in peers:
        pl.semaphore_signal(barrier, inc=1, device_id=peer, device_id_type=MESH)

    small = [
        pltpu.make_async_copy(src, dst, load_sem.at[14 + i])
        for i, (src, dst) in enumerate([
            (tokens_in, tokens), (mgain_in, mgain), (wq_in_hbm, wq), (ids_in, ids), (rw_in, rw),
            (wo_in_hbm, wo), (lens_in, lens), (hoff_in, hoff), (egain_in, egain),
        ])
    ]
    for copy in small:
        copy.start()
    loads = [(key, kbuf), (val, vbuf)]
    for t in range(nx):
        loads += [(gate.at[:, t], gbuf.at[t]), (up.at[:, t], ubuf.at[t])]
    for t in range(nx):
        loads += [(down.at[:, pl.ds(t * d.xs, d.xs)], dbuf.at[t])]
    loads = [
        pltpu.make_async_copy(src, dst, load_sem.at[23 + i]) for i, (src, dst) in enumerate(loads)
    ]
    for copy in loads:
        copy.start()
    small[2].wait()
    pl.semaphore_wait(barrier, len(peers))
    pending = []

    def send(copy):
        copy.start()
        pending.append(copy)
        return copy

    def keep(number, src, dst):
        copy = pltpu.make_async_copy(src, dst, load_sem.at[number])
        copy.start()
        return copy

    own_rows = pl.multiple_of(y * d.rp, 8)
    own_piece = pl.multiple_of((y * nc + c) * d.rp, 8)
    wq_in = [
        send(remote(wq, wq_all.at[pl.ds(own_rows, d.rp)], ys.at[k], yr.at[k], y=up_y(k)))
        for k in far_first(ny)
    ]
    own_q = keep(5, wq, wq_all.at[pl.ds(own_rows, d.rp)])
    for copy in small[:2] + small[3:]:
        copy.wait()

    wide = tokens[...].astype(F32)
    scale = lax.rsqrt(jnp.mean(wide * wide, axis=1, keepdims=True) + 1e-06)
    normed = (wide * scale * mgain[...]).astype(BF16).astype(F32)
    filler = jnp.zeros((PAD - b, d.width), F32)
    normed = jnp.concatenate([normed, filler], axis=0)
    plain = jnp.concatenate([wide, filler], axis=0).astype(BF16)
    for t in range(nz):
        ta_send[t] = plain[:, t * d.zb : (t + 1) * d.zb]
    share = ny * d.rp
    depth, tall = d.rp.bit_length() - 1, share.bit_length() - 1
    to = iota((d.zb, d.zb), 1)
    source = ((((to & (share - 1)) >> depth) * nc + (to >> tall)) << depth) + (to & (d.rp - 1))
    order = onehot(iota((d.zb, d.zb), 0) == source)
    moved = dot(
        jnp.concatenate([normed[:, t * d.zb : (t + 1) * d.zb] for t in range(nz)], axis=0).astype(BF16),
        order).astype(BF16)
    for t in range(nz):
        for j in range(nc):
            qa_send[t * nc + j] = moved[t * PAD : (t + 1) * PAD, j * share : (j + 1) * share]
    lane = iota((4, 128), 1)
    field = iota((4, 128), 0)
    info = jnp.zeros((4, 128), F32)
    for r in range(b):
        here = lane == z * b + r
        for j, number in enumerate((
            ids[0, r].astype(F32), ids[1, r].astype(F32), rw[0, r], rw[1, r],
        )):
            info = jnp.where(here & (field == j), number, info)
    info_a[...] = info
    zc = [(k, j) for k in far_first(nz) for j in range(nc)] + [(0, j) for j in range(1, nc)]
    me = z * nc + c

    def there(k, j):
        return up_z(k) * nc + up_c(j)

    def zc_exchange(base, source, everything):
        return [
            send(remote(
                source.at[there(k, j)], everything.at[me],
                zs.at[base + k * nc + j], zr.at[base + k * nc + j], z=up_z(k), c=up_c(j)))
            for k, j in zc
        ]

    def from_y(k):
        return lax.rem(y - k + ny, ny)

    qa_in = zc_exchange(0, qa_send, qa_recv)
    own_a = keep(7, qa_send.at[me], qa_recv.at[me])
    info_in = [
        send(remote(info_a, info_az.at[z], zs.at[4 * nz + k], zr.at[4 * nz + k], z=up_z(k)))
        for k in far_first(nz)
    ]
    for copy in qa_in:
        copy.wait_recv()
    own_a.wait()
    own_q.wait()
    rows_a = stacked(qa_recv, nz * nc)
    part = d.ql // PAD
    for copy in wq_in:
        copy.wait_recv()
    partial = dot(rows_a, wq_all[...])
    fourth = (iota((nz * nc * PAD, 1), 0) & (PAD - 1)) == b
    last = partial[:, b * part :]
    for r in range(b):
        span = slice(r * part, (r + 1) * part)
        packed = jnp.where(fourth, pltpu.roll(last, b - r, 0), partial[:, span]).astype(BF16)
        for t in range(nz * nc):
            qp_send[t, :, span] = packed[t * PAD : (t + 1) * PAD]
    qp_in = zc_exchange(2 * nz, qp_send, qp_recv)
    own_p = keep(9, qp_send.at[me], qp_recv.at[me])
    wo_in = {
        k: send(remote(wo, wo_all.at[pl.ds(own_piece, d.rp)], ys.at[ny + k], yr.at[ny + k], y=up_y(k)))
        for k in far_first(ny)
    }
    own_o = keep(6, wo, wo_all.at[pl.ds(own_piece, d.rp)])
    wo_fwd = [send(remote(wo, wo_all.at[pl.ds(own_piece, d.rp)], cs.at[0], cr.at[0], c=other))]
    ta_in = [
        send(remote(ta_send.at[up_z(k)], ta_recv.at[z], zs.at[5 * nz + k], zr.at[5 * nz + k], z=up_z(k)))
        for k in far_first(nz)
    ]
    own_t = keep(8, ta_send.at[z], ta_recv.at[z])

    for copy in info_in:
        copy.wait_recv()
    info = info_a[...]
    for k in range(1, nz):
        info = info + info_az[up_z(k)]
    info_by[y] = info
    info_b[...] = info
    info_y_in = [
        send(remote(info_b, info_by.at[y], ys.at[2 * ny + k], yr.at[2 * ny + k], y=up_y(k)))
        for k in far_first(ny)
    ]
    loads[0].wait()
    loads[1].wait()

    for copy in qp_in:
        copy.wait_recv()
    own_p.wait()
    q = qp_recv[0].astype(F32)
    for t in range(1, nz * nc):
        q = q + qp_recv[t].astype(F32)
    last = [q[b : b + 1, r * part : (r + 1) * part] for r in range(b)]
    last = jnp.concatenate(last + [jnp.zeros((PAD - b, part), F32)], axis=0)
    q = jnp.concatenate([q, last], axis=1)
    mixed = attention(d, q, kbuf, vbuf, lens, hoff)
    mx_send[...] = mixed
    mx_in = [
        send(remote(mx_send, mx_recv.at[z], zs.at[6 * nz + k], zr.at[6 * nz + k], z=up_z(k)))
        for k in far_first(nz)
    ]
    own_m = keep(10, mx_send, mx_recv.at[z])

    for copy in info_y_in:
        copy.wait_recv()
    info_c_in = send(remote(info_by, info_cc, cs.at[ny], cr.at[ny], c=other))

    for k in near_first(ny):
        wo_in[k].wait_recv()
        part = wo_all.at[pl.ds(pl.multiple_of((from_y(k) * nc + c) * d.rp, 8), d.rp)]
        wo_fwd.append(send(remote(part, part, cs.at[k], cr.at[k], c=other)))
    pick_t = iota((line, nz * PAD), 0)
    pick_s = iota((line, nz * PAD), 1)
    within = pick_s & (PAD - 1)
    pick = onehot((within < b) & ((pick_s >> (PAD.bit_length() - 1)) * b + within == pick_t))
    for copy in ta_in:
        copy.wait_recv()
    own_t.wait()
    tok = dot(pick, stacked(ta_recv, nz))
    count = float(ny * nc)
    own_ids = info_b[...][0:1, :line]
    zone = iota((8, line), 0).astype(F32) * count
    bound = onehot((own_ids >= zone) & (own_ids < zone + count))
    bound_rank = dot(bound, onehot(iota((line, line), 0) < iota((line, line), 1)))
    wide_rows = nz * SLOTS // 2
    widen = onehot((iota((wide_rows, 8), 0) >> 3) == iota((wide_rows, 8), 1))
    bound = dot(widen, bound) > 0.5
    bound_rank = dot(widen, bound_rank.astype(BF16))
    number = (iota((wide_rows, line), 0) & 7).astype(F32)
    pack_all = jnp.concatenate(
        [onehot(bound & (bound_rank == number)), onehot(bound & (bound_rank == number + 8.0))], axis=0)
    moved = dot(pack_all, tok.astype(BF16))
    for t, part in enumerate(side_by_side(d, moved[:wide_rows], moved[wide_rows:])):
        tk_all[t] = part.reshape(nz, SLOTS // 2, 128)
    tk_in = [
        send(remote(tk_all.at[x, up_z(k)], tk_recv.at[z], zs.at[9 * nz + k], zr.at[9 * nz + k], z=up_z(k)))
        for k in far_first(nz)
    ]
    own_tk = keep(0, tk_all.at[x, z], tk_recv.at[z])
    pack_all = dot(pack_all, pick).astype(BF16)
    for t in range(nx):
        gains[t] = jnp.concatenate(
            [egain[:, u * d.zb + t * 64 : u * d.zb + t * 64 + 64] for u in range(nz)], axis=1)
    for copy in wo_fwd:
        copy.wait_recv()
    own_o.wait()
    for copy in mx_in:
        copy.wait_recv()
    own_m.wait()
    all_mixed = stacked(mx_recv, nz)
    moved = dot(dot(pack_all, all_mixed).astype(BF16), wo_all[...], ((1,), (1,)))
    for t, part in enumerate(side_by_side(d, moved[:wide_rows], moved[wide_rows:])):
        f_send[t] = part.reshape(nz, SLOTS // 2, 128)
    f_in = [
        send(remote(
            f_send.at[up_x(j), up_z(k)], f_recv.at[x, z],
            fs.at[k * nx + j], fr.at[k * nx + j], x=up_x(j), z=up_z(k)))
        for k in far_first(nz) + [0] for j in far_first(nx) + [0] if k or j
    ]
    own_f = keep(1, f_send.at[x, z], f_recv.at[x, z])
    tight = dot(pick, all_mixed).astype(BF16)
    pt_send[...] = dot(tight, wo_all[...], ((1,), (1,))).astype(BF16)

    away = remote(pt_send, pt_recv.at[x], xs.at[0], xr.at[x], x=home)
    own_lanes = pl.multiple_of(lax.rem(z, d.nb) * d.zb, d.zb)
    own_block = line_rows.at[:, pl.ds(own_lanes, d.zb)]
    own_b = pltpu.make_async_copy(rb_send, own_block, load_sem.at[11])

    def to_line(k):
        return remote(
            rb_send, own_block, zs.at[7 * nz + k], zr.at[7 * nz + lax.rem(z, d.nb)], z=up_z(k))

    @pl.when(x != home)
    def _():
        away.start()

    info_c_in.wait_recv()
    near = [info_by[t] for t in range(ny)]
    far = [info_cc[t] for t in range(ny)]
    info = jnp.concatenate(
        [jnp.where(c == 0, u, v)[:, :line] for u, v in zip(near, far)]
        + [jnp.where(c == 0, v, u)[:, :line] for u, v in zip(near, far)], axis=1)
    info_out[...] = info
    id0 = info[0:1]
    id1 = info[1:2]
    low = z.astype(F32) * count
    half_width = ny * line

    def line_of(places):
        return jnp.floor((places.astype(F32) + 0.5) * (1.0 / line))

    token_line = line_of(iota((1, d.nt), 1))
    token_half = jnp.where(token_line >= ny, 1.0, 0.0)
    ours = token_half == c.astype(F32)
    staying = (id0 >= low) & (id0 < low + count)
    stay = jnp.where(staying, 1.0, 0.0)
    hits = []
    for j in range(nc):
        expert = low + (y * nc + j).astype(F32)
        hits.append((jnp.where(id0 == expert, 1.0, 0.0), jnp.where(id1 == expert, 1.0, 0.0)))
    first, second = iota((d.nt, d.nt), 0), iota((d.nt, d.nt), 1)
    earlier = first < second
    same_line = line_of(first) == line_of(second)
    same_half = (first < half_width) == (second < half_width)
    line_rank = dot(jnp.broadcast_to(stay, (8, d.nt)).astype(BF16), onehot(earlier & same_line))[0:1]
    hit_rows = jnp.concatenate([h0 + h1 for h0, h1 in hits], axis=0)
    hit_rank = dot(hit_rows.astype(BF16), onehot(earlier & same_half))
    numbers = iota((SLOTS, d.nt), 0).astype(F32)
    chosen = [
        onehot((numbers == hit_rank[j : j + 1]) & (hit_rows[j : j + 1] > 0.5) & ours) for j in range(nc)
    ]
    routes = [h0 * info[2:3] + h1 * info[3:4] for h0, h1 in hits]
    slot_route = jnp.concatenate([
        jnp.sum(chosen[j].astype(F32) * routes[j], axis=1, keepdims=True) for j in range(nc)], axis=0)
    chosen = jnp.concatenate(chosen, axis=0)
    kept = ny * SLOTS
    place = (token_line - c.astype(F32) * ny) * SLOTS + line_rank
    packed = onehot(
        (iota((kept, d.nt), 0).astype(F32) == place) & staying & ours & (line_rank < SLOTS - 0.5))
    chosen_tokens = chosen
    chosen = dot(chosen, packed, ((1,), (1,))).astype(BF16)
    owner_s = iota((ny * nz * PAD, d.nt), 0)
    owner_t = iota((ny * nz * PAD, d.nt), 1) - c * half_width
    r_of = owner_s & (PAD - 1)
    owner_i = owner_s >> (PAD.bit_length() - 1)
    first_of = (owner_i & (ny - 1)) * line + (owner_i >> (ny.bit_length() - 1)) * b
    owners = onehot((r_of < b) & (first_of + r_of == owner_t))
    owners = dot(owners, chosen_tokens, ((1,), (1,)))
    homes = []
    for r in range(b):
        last = onehot((r_of == b) & (first_of + r == owner_t))
        last = dot(last, chosen_tokens, ((1,), (1,)))
        homes.append(jnp.concatenate([owners, last], axis=1).astype(BF16))
    expert = iota((d.experts, d.nt), 0).astype(F32)
    named = onehot((id0 == expert) | (id1 == expert))
    group_t = iota((d.nt, 128), 0)
    group_g = iota((d.nt, 128), 1)
    halves = dot(named, onehot((group_t >= half_width) == (group_g > 0)))
    zone = iota((8, d.nt), 0).astype(F32) * count
    lines = dot(onehot((id0 >= zone) & (id0 < zone + count)), onehot(line_of(group_t) == group_g.astype(F32)))
    most = jnp.maximum(jnp.max(halves), jnp.max(lines))
    most_out[0] = jnp.where(most > SLOTS, 1, 0)

    own_tk.wait()
    for copy in tk_in:
        copy.wait_recv()
    own_f.wait()
    for copy in f_in:
        copy.wait_recv()
    summed = []
    for u in range(nz):
        total = tk_recv[u].astype(F32)
        for t in range(nx):
            total = total + f_recv[t, u].astype(F32)
        summed.append(total)
    low_lanes = iota((SLOTS // 2, 128), 1) < 64
    for u in range(0, nz, 2):
        span = slice(u * 64, u * 64 + 128)
        own_send[:, span] = jnp.concatenate([
            jnp.where(low_lanes, summed[u], turned(summed[u + 1])),
            jnp.where(low_lanes, turned(summed[u]), summed[u + 1])], axis=0).astype(BF16)
    own_slots = pl.ds(pl.multiple_of(y * SLOTS, SLOTS), SLOTS)
    rows_in = [
        send(remote(own_send, rows.at[own_slots], ys.at[3 * ny + k], yr.at[3 * ny + k], y=up_y(k)))
        for k in far_first(ny)
    ]
    own_s = keep(13, own_send, rows.at[own_slots])
    @pl.when(x == home)
    def _():
        total = tok + pt_send[...].astype(F32)
        for k in range(1, nx):
            source = lax.rem(x + k, nx)
            remote(pt_send, pt_recv.at[source], xs.at[0], xr.at[source], x=source).wait_recv()
            total = total + pt_recv[source].astype(F32)
        rb_send[...] = total.astype(BF16)
        own_b.start()
        for k in far_first(nz):
            to_line(k).start()

    own_s.wait()
    for copy in rows_in:
        copy.wait_recv()

    s_send[...] = dot(chosen, rows[...]).astype(BF16).reshape(nc, SLOTS, d.xs)
    xc = [(k, j) for k in far_first(nx) for j in range(nc)] + [(0, j) for j in range(1, nc)]
    our_slots = pl.ds(pl.multiple_of(c * SLOTS, SLOTS), SLOTS)
    s_in = [
        send(remote(
            s_send.at[up_c(j)], s_recv.at[x, our_slots],
            xs.at[1 + k * nc + j], xr.at[nx + k * nc + j], x=up_x(k), c=up_c(j)))
        for k, j in xc
    ]
    own_s = keep(5, s_send.at[c], s_recv.at[x, our_slots])
    for copy in loads[2:]:
        copy.wait()
    gated = jnp.zeros((nc * SLOTS, d.ff), F32)
    upward = jnp.zeros((nc * SLOTS, d.ff), F32)
    square = jnp.zeros((nc * SLOTS, 1), F32)
    waiting = dict(zip(xc, s_in))
    own_s.wait()
    for k in [0] + near_first(nx):
        for j in range(nc):
            if k or j:
                waiting[(k, j)].wait_recv()
        t = lax.rem(x - k + nx, nx)
        part = s_recv[t].astype(F32)
        square = square + jnp.sum(part * part, axis=1, keepdims=True)
        part = (part * gains[t]).astype(BF16)
        gated = gated + dot(part, gbuf[t].reshape(d.xs, d.ff))
        upward = upward + dot(part, ubuf[t].reshape(d.xs, d.ff))
    scale = lax.rsqrt(square / d.width + 1e-06)
    gated = gated * scale
    hidden = (gated / (1.0 + jnp.exp(-gated)) * (upward * scale)).astype(BF16)

    def to_half(j):
        return pl.ds(pl.multiple_of(up_c(j) * SLOTS, SLOTS), SLOTS)

    h_in = []
    for k in far_first(nx) + [0]:
        h_send[up_x(k)] = dot(hidden, dbuf[up_x(k)]).astype(BF16)
        for j in range(nc):
            if k or j:
                h_in.append(send(remote(
                    h_send.at[up_x(k), to_half(j)], h_recv.at[x, our_slots],
                    xs.at[1 + nx * nc + k * nc + j], xr.at[nx + nx * nc + k * nc + j],
                    x=up_x(k), c=up_c(j))))
    own_h = keep(6, h_send.at[x, our_slots], h_recv.at[x, our_slots])
    own_h.wait()
    for copy in h_in:
        copy.wait_recv()
    total = h_recv[0].astype(F32)
    for t in range(1, nx):
        total = total + h_recv[t].astype(F32)
    answer = total.astype(BF16).astype(F32) * slot_route
    part = d.xs // PAD
    pairs = [
        jnp.concatenate([answer[:, r * part : (r + 1) * part], answer[:, b * part :]], axis=0).astype(BF16)
        for r in range(b)
    ]

    def give(t, k):
        return remote(
            y_send.at[t * ny + up_y(k)], y_recv.at[y * nz + z],
            gs.at[t * ny + k], gr.at[z * ny + k], z=t, y=up_y(k))

    some = nz // 2
    for first_z in range(0, nz, some):
        area = slice(first_z * ny, (first_z + some) * ny)
        for r in range(b):
            from_home = homes[r][area.start * PAD : area.stop * PAD]
            y_send[area, :, r * part : (r + 1) * part] = (
                dot(from_home, pairs[r]).reshape(some * ny, PAD, part).astype(BF16))
        for t in range(first_z, first_z + some):
            for k in far_first(ny):
                send(give(t, k))

            @pl.when(z != t)
            def _():
                give(t, 0).start()

    given = nz * (ny - 1)
    own_y = keep(7, y_send.at[z * ny + y], y_recv.at[y * nz + z])
    for j in range(d.nb):
        source = x * d.nb + j

        @pl.when(z != source)
        def _():
            block = line_rows.at[:, pl.ds(j * d.zb, d.zb)]
            remote(rb_send, block, zs.at[0], zr.at[7 * nz + j], z=source).wait_recv()

    @pl.when(x == home)
    def _():
        own_b.wait()

    save = keep(12, line_rows, line_out)
    mine_t = iota((8, line), 1)
    mine_r = iota((8, line), 0)
    resid = dot(onehot((mine_r < b) & (mine_t == mine_r + z * b)), line_rows[...])
    save.wait()

    @pl.when(x != home)
    def _():
        away.wait_send()

    @pl.when(x == home)
    def _():
        for k in near_first(nz):
            to_line(k).wait_send()

    for copy in pending[:-given]:
        copy.wait_send()
    own_y.wait()
    for t in range(nz):
        for k in near_first(ny):
            remote(
                y_send.at[0], y_recv.at[from_y(k) * nz + t], gs.at[0], gr.at[t * ny + k],
                z=t, y=from_y(k)).wait_recv()

        @pl.when(z != t)
        def _():
            remote(
                y_send.at[0], y_recv.at[y * nz + t], gs.at[0], gr.at[t * ny], z=t).wait_recv()

    total = y_recv[0].astype(F32)
    for t in range(1, ny * nz):
        total = total + y_recv[t].astype(F32)
    last = jnp.concatenate([total[b : b + 1, r * part : (r + 1) * part] for r in range(b)], axis=0)
    out[...] = (resid[0:b] + jnp.concatenate([total[0:b], last], axis=1)).astype(BF16)
    for t in range(nz):
        @pl.when(z != t)
        def _():
            give(t, 0).wait_send()

    for copy in pending[-given:]:
        copy.wait_send()


def layer(d, args):
    def vmem(*shape, dtype=BF16):
        return pltpu.VMEM(shape, dtype)

    line = d.nz * d.b
    dma = pltpu.SemaphoreType.DMA
    inside = pl.BlockSpec(memory_space=pltpu.VMEM)
    outside = pl.BlockSpec(memory_space=pltpu.HBM)
    return pl.pallas_call(
        functools.partial(kernel, d),
        out_shape=(
            pltpu.VMEM((d.b, d.xs), BF16),
            jax.ShapeDtypeStruct((line, d.xs), BF16),
            pltpu.VMEM((4, d.nt), F32),
            pltpu.SMEM((1,), jnp.int32),
        ),
        in_specs=[outside] * 14,
        out_specs=(inside, outside, inside, pl.BlockSpec(memory_space=pltpu.SMEM)),
        scratch_shapes=[
            vmem(d.b, d.width), vmem(1, d.width, dtype=F32), vmem(d.rp, d.ql), vmem(d.rp, d.ql),
            vmem(1, d.width, dtype=F32),
            pltpu.SMEM((d.b,), jnp.int32), pltpu.SMEM((d.ql // d.hd,), F32),
            pltpu.SMEM((2, d.b), jnp.int32), pltpu.SMEM((2, d.b), F32),
            vmem(d.b, d.cache, d.hd), vmem(d.b, d.cache, d.hd),
            vmem(d.nx, d.nz, d.zb // d.nx, d.ff), vmem(d.nx, d.nz, d.zb // d.nx, d.ff), vmem(d.nx, d.ff, d.xs),
            dma((25 + 3 * d.nx,)),
            vmem(d.nz, PAD, d.zb), vmem(d.nz, PAD, d.zb),
            vmem(d.nz * d.nc, PAD, d.zb // d.nc), vmem(d.nz * d.nc, PAD, d.zb // d.nc),
            vmem(d.ny * d.rp, d.ql), vmem(d.zb, d.ql),
            vmem(d.nz * d.nc, PAD, d.ql // PAD * d.b), vmem(d.nz * d.nc, PAD, d.ql // PAD * d.b),
            vmem(PAD, d.ql), vmem(d.nz, PAD, d.ql),
            vmem(d.nx, d.nz, SLOTS // 2, 128), vmem(d.nz, SLOTS // 2, 128),
            vmem(d.nx, d.nz, SLOTS // 2, 128), vmem(d.nx, d.nz, SLOTS // 2, 128),
            vmem(d.nx, 1, d.xs, dtype=F32),
            vmem(line, d.zb), vmem(d.nx, line, d.zb), vmem(line, d.zb),
            vmem(line, d.xs), vmem(SLOTS, d.xs), vmem(d.ny * SLOTS, d.xs),
            vmem(d.nc, SLOTS, d.xs), vmem(d.nx, d.nc * SLOTS, d.xs),
            vmem(d.nx, d.nc * SLOTS, d.xs), vmem(d.nx, d.nc * SLOTS, d.xs),
            vmem(d.ny * d.nz, PAD, d.xs // PAD * d.b), vmem(d.ny * d.nz, PAD, d.xs // PAD * d.b),
            vmem(4, 128, dtype=F32), vmem(d.nz, 4, 128, dtype=F32), vmem(4, 128, dtype=F32),
            vmem(d.ny, 4, 128, dtype=F32), vmem(d.ny, 4, 128, dtype=F32),
            dma((10 * d.nz,)), dma((10 * d.nz,)),
            dma((5 * d.ny,)), dma((5 * d.ny,)),
            dma((1 + 2 * d.nx * d.nc,)), dma((d.nx + 2 * d.nx * d.nc,)),
            dma((d.ny + 1,)), dma((d.ny + 1,)),
            dma((d.nz * d.nx,)), dma((d.nz * d.nx,)),
            dma((d.nz * d.ny,)), dma((d.nz * d.ny,)),
        ],
        compiler_params=pltpu.CompilerParams(
            collective_id=0, has_side_effects=True, vmem_limit_bytes=60 * 1024 * 1024),
    )(*args)


def crowded(d, line, info, expert_gain, gate_weight, up_weight, down_weight):
    places = ("c", "y")
    copies = jnp.broadcast_to(line, (d.nc * d.ny, *line.shape))
    lines = lax.all_to_all(copies, places, split_axis=0, concat_axis=0, tiled=True)
    rows = lines.reshape(d.nt, d.xs)
    copies = jnp.broadcast_to(rows, (d.nx, *rows.shape))
    spans = lax.all_to_all(copies, "x", split_axis=0, concat_axis=0, tiled=True)
    full = jnp.moveaxis(spans, 0, 1).reshape(d.nt, d.width)
    wide = full.astype(F32)
    scale = lax.rsqrt(jnp.mean(wide * wide, axis=-1, keepdims=True) + 1e-06)
    normed = (wide * scale * expert_gain).astype(BF16)
    gated = jnp.dot(normed, gate_weight, preferred_element_type=F32)
    upward = jnp.dot(normed, up_weight, preferred_element_type=F32)
    hidden = (jax.nn.silu(gated) * upward).astype(BF16)
    term = jnp.dot(hidden, down_weight, preferred_element_type=F32).astype(BF16)
    tiles = jnp.moveaxis(term.reshape(d.nt, d.nx, d.xs), 1, 0)
    terms = lax.all_to_all(tiles, "x", split_axis=0, concat_axis=0, tiled=True)
    answer = terms.astype(F32).sum(axis=0).astype(BF16).astype(F32)
    mine = lax.axis_index(EP).astype(F32)
    route = jnp.where(info[0] == mine, info[2], 0.0) + jnp.where(info[1] == mine, info[3], 0.0)
    answer = answer * route[:, None]
    answer = answer.reshape(d.nc, d.ny, d.nz, d.b, d.xs).transpose(2, 1, 0, 3, 4)
    answer = answer.reshape(-1, d.b, d.xs)
    back = lax.all_to_all(answer, EP, split_axis=0, concat_axis=0, tiled=True)
    z, y, c = (lax.axis_index(name) for name in EP)
    first = ((c * d.ny + y) * d.nz + z) * d.b
    resid = lax.dynamic_slice_in_dim(rows, first, d.b, 0)
    return (resid.astype(F32) + back.sum(axis=0)).astype(BF16)


def local(
    tokens,
    mixer_gain,
    query_weight,
    key_cache,
    value_cache,
    seq_lengths,
    head_offset,
    output_weight,
    expert_gain,
    expert_ids,
    route_weight,
    gate_weight,
    up_weight,
    down_weight,
):
    nz, ny, nc, nx = (lax.axis_size(name) for name in ("z", "y", "c", "x"))
    batch, width = tokens.shape
    d = SimpleNamespace(
        nz=nz, ny=ny, nc=nc, nx=nx, b=batch, width=width, zb=width // nz, xs=width // nx,
        nb=nz // nx, rp=query_weight.shape[0], ql=query_weight.shape[1], hd=key_cache.shape[3],
        cache=key_cache.shape[1], ff=gate_weight.shape[2], nt=nz * ny * nc * batch,
        experts=nz * ny * nc,
    )
    done, line, info, most = layer(d, (
        tokens,
        mixer_gain.reshape(1, width),
        query_weight,
        key_cache.reshape(batch, d.cache, d.hd),
        value_cache.reshape(batch, d.cache, d.hd),
        seq_lengths,
        head_offset,
        output_weight.T,
        expert_gain.reshape(1, width),
        expert_ids.T,
        route_weight.T,
        gate_weight.reshape(nz, nx, d.zb // nx, d.ff),
        up_weight.reshape(nz, nx, d.zb // nx, d.ff),
        down_weight[0],
    ))
    return lax.cond(
        most[0] > 0,
        lambda: crowded(d, line, info, expert_gain, gate_weight[0], up_weight[0], down_weight[0]),
        lambda: done,
    )


def solution(mesh):
    split = Mesh(mesh.devices.reshape(8, 8, 2, mesh.shape["tp"]), ("z", "y", "c", "x"))
    return sharded(split)


def sharded(split):
    in_specs = (
        P(EP, None),
        P(),
        P(EP, "x"),
        P(EP, None, "x", None),
        P(EP, None, "x", None),
        P(EP),
        P("x"),
        P("x", EP),
        P(),
        P(EP, None),
        P(EP, None),
        P(EP, None, "x"),
        P(EP, None, "x"),
        P(EP, "x", None),
    )
    return jax.shard_map(local, mesh=split, in_specs=in_specs, out_specs=P(EP, "x"), check_vma=False)
```

```python
import functools
from types import SimpleNamespace

import jax
import jax.numpy as jnp
from jax import lax
from jax.experimental import pallas as pl
from jax.experimental.pallas import tpu as pltpu
from jax.sharding import Mesh
from jax.sharding import PartitionSpec as P

EP = ("z", "y", "c")
SLOTS = 16
PAD = 4
F32 = jnp.float32
BF16 = jnp.bfloat16


def iota(shape, dim):
    return lax.broadcasted_iota(jnp.int32, shape, dim)


def dot(a, b, dims=((1,), (0,)), precision=None):
    return lax.dot_general(a, b, (dims, ((), ())), precision=precision, preferred_element_type=F32)


def onehot(condition):
    return jnp.where(condition, 1.0, 0.0).astype(BF16)


def near_first(count):
    return sorted(range(1, count), key=lambda k: min(k, count - k))


def far_first(count):
    return near_first(count)[::-1]


def stacked(ref, count):
    return jnp.concatenate([ref[t].astype(F32) for t in range(count)], axis=0).astype(BF16)


def turned(value):
    return jnp.concatenate([value[:, 64:], value[:, :64]], axis=1)


def side_by_side(d, upper, lower):
    low = iota((upper.shape[0], 128), 1) < 64
    result = []
    for t in range(d.nx):
        span = slice(t // 2 * 128, t // 2 * 128 + 128)
        left, right = upper[:, span], lower[:, span]
        pair = (left, turned(right)) if t % 2 == 0 else (turned(left), right)
        result.append(jnp.where(low, *pair).astype(BF16))
    return result


def remote(src, dst, send_sem, recv_sem, **where):
    return pltpu.make_async_remote_copy(
        src_ref=src,
        dst_ref=dst,
        send_sem=send_sem,
        recv_sem=recv_sem,
        device_id=where,
        device_id_type=pl.DeviceIdType.MESH,
    )


def attention(d, q, kbuf, vbuf, lens, hoff):
    heads = d.ql // d.hd
    rows = heads * PAD
    queries = jnp.concatenate([q[:, h * d.hd : (h + 1) * d.hd] for h in range(heads)], axis=0)
    queries = queries.astype(BF16)
    row = iota((rows, 1), 0)
    seq = row & (PAD - 1)
    head = row >> (PAD.bit_length() - 1)
    score = jnp.zeros((rows, d.cache), F32)
    length = jnp.zeros((rows, 1), jnp.int32)
    offset = jnp.zeros((rows, 1), F32)
    for b in range(d.b):
        one = dot(queries, kbuf[b], ((1,), (1,)))
        score = jnp.where(seq == b, one, score)
        length = jnp.where(seq == b, lens[b], length)
    for h in range(heads):
        offset = jnp.where(head == h, hoff[h], offset)
    score = score * (d.hd**-0.5) + offset
    valid = iota((rows, d.cache), 1) < length
    soft = jnp.log1p(jnp.exp(-jnp.abs(score)))
    log_take = jnp.minimum(score, 0.0) - soft
    log_pass = jnp.where(valid, jnp.minimum(-score, 0.0) - soft, 0.0)
    blocks = d.cache // 128
    pieces = [log_pass[:, i * 128 : (i + 1) * 128] for i in range(blocks)]
    after = (iota((128, 128), 0) > iota((128, 128), 1)).astype(F32)
    inside = dot(jnp.concatenate(pieces, axis=0), after, precision=lax.Precision.HIGHEST)
    later = jnp.zeros((rows, 1), F32)
    sums = [None] * blocks
    for i in range(blocks - 1, -1, -1):
        sums[i] = inside[i * rows : (i + 1) * rows] + later
        later = later + jnp.sum(pieces[i], axis=1, keepdims=True)
    weight = jnp.where(valid, jnp.exp(log_take + jnp.concatenate(sums, axis=1)), 0.0).astype(BF16)
    total = jnp.zeros((rows, d.hd), F32)
    for b in range(d.b):
        total = jnp.where(seq == b, dot(weight, vbuf[b]), total)
    return jnp.concatenate([total[h * PAD : (h + 1) * PAD] for h in range(heads)], axis=1).astype(BF16)


def kernel(d, *refs):
    (tokens_in, mgain_in, wq_in_hbm, key, val, lens_in, hoff_in, wo_in_hbm, egain_in, ids_in, rw_in,
     gate, up, down) = refs[:14]
    out, line_out, info_out, most_out = refs[14:18]
    (tokens, mgain, wq, wo, egain, lens, hoff, ids, rw,
     kbuf, vbuf, gbuf, ubuf, dbuf, load_sem,
     ta_send, ta_recv, qa_send, qa_recv, wq_all, wo_all, qp_send, qp_recv, mx_send, mx_recv,
     tk_all, tk_recv, f_send, f_recv, gains,
     pt_send, pt_recv, rb_send, line_rows, own_send, rows, s_send, s_recv, h_send, h_recv,
     y_send, y_recv,
     info_a, info_az, info_b, info_by, info_cc,
     zs, zr, ys, yr, xs, xr, cs, cr, fs, fr, gs, gr) = refs[18:]
    z, y, c, x = (lax.axis_index(name) for name in ("z", "y", "c", "x"))
    nz, ny, nc, nx, b = d.nz, d.ny, d.nc, d.nx, d.b
    other = 1 - c
    slot = c * ny + y
    line = nz * b
    home = z // d.nb
    MESH = pl.DeviceIdType.MESH

    def up_z(k):
        return lax.rem(z + k, nz)

    def up_y(k):
        return lax.rem(y + k, ny)

    def up_x(k):
        return lax.rem(x + k, nx)

    def up_c(k):
        return lax.rem(c + k, nc)

    barrier = pltpu.get_barrier_semaphore()
    peers = [{"z": up_z(k), "c": up_c(j)} for k in far_first(nz) for j in range(nc)]
    peers += [{"y": up_y(k)} for k in far_first(ny)]
    peers += [{"x": up_x(k), "c": up_c(j)} for k in far_first(nx) for j in range(nc)]
    peers += [{"c": other}]
    for peer in peers:
        pl.semaphore_signal(barrier, inc=1, device_id=peer, device_id_type=MESH)

    small = [
        pltpu.make_async_copy(src, dst, load_sem.at[14 + i])
        for i, (src, dst) in enumerate([
            (tokens_in, tokens), (mgain_in, mgain), (wq_in_hbm, wq), (ids_in, ids), (rw_in, rw),
            (wo_in_hbm, wo), (lens_in, lens), (hoff_in, hoff), (egain_in, egain),
        ])
    ]
    for copy in small:
        copy.start()
    loads = [(key, kbuf), (val, vbuf)]
    for t in range(nx):
        loads += [(gate.at[:, t], gbuf.at[t]), (up.at[:, t], ubuf.at[t])]
    for t in range(nx):
        loads += [(down.at[:, pl.ds(t * d.xs, d.xs)], dbuf.at[t])]
    loads = [
        pltpu.make_async_copy(src, dst, load_sem.at[23 + i]) for i, (src, dst) in enumerate(loads)
    ]
    for copy in loads:
        copy.start()
    small[2].wait()
    pl.semaphore_wait(barrier, len(peers))
    pending = []

    def send(copy):
        copy.start()
        pending.append(copy)
        return copy

    def keep(number, src, dst):
        copy = pltpu.make_async_copy(src, dst, load_sem.at[number])
        copy.start()
        return copy

    own_rows = pl.multiple_of(y * d.rp, 8)
    own_piece = pl.multiple_of((y * nc + c) * d.rp, 8)
    wq_in = [
        send(remote(wq, wq_all.at[pl.ds(own_rows, d.rp)], ys.at[k], yr.at[k], y=up_y(k)))
        for k in far_first(ny)
    ]
    own_q = keep(5, wq, wq_all.at[pl.ds(own_rows, d.rp)])
    for copy in small[:2] + small[3:]:
        copy.wait()

    wide = tokens[...].astype(F32)
    scale = lax.rsqrt(jnp.mean(wide * wide, axis=1, keepdims=True) + 1e-06)
    normed = (wide * scale * mgain[...]).astype(BF16).astype(F32)
    filler = jnp.zeros((PAD - b, d.width), F32)
    normed = jnp.concatenate([normed, filler], axis=0)
    plain = jnp.concatenate([wide, filler], axis=0).astype(BF16)
    for t in range(nz):
        ta_send[t] = plain[:, t * d.zb : (t + 1) * d.zb]
    share = ny * d.rp
    depth, tall = d.rp.bit_length() - 1, share.bit_length() - 1
    to = iota((d.zb, d.zb), 1)
    source = ((((to & (share - 1)) >> depth) * nc + (to >> tall)) << depth) + (to & (d.rp - 1))
    order = onehot(iota((d.zb, d.zb), 0) == source)
    moved = dot(
        jnp.concatenate([normed[:, t * d.zb : (t + 1) * d.zb] for t in range(nz)], axis=0).astype(BF16),
        order).astype(BF16)
    for t in range(nz):
        for j in range(nc):
            qa_send[t * nc + j] = moved[t * PAD : (t + 1) * PAD, j * share : (j + 1) * share]
    lane = iota((4, 128), 1)
    field = iota((4, 128), 0)
    info = jnp.zeros((4, 128), F32)
    for r in range(b):
        here = lane == z * b + r
        for j, number in enumerate((
            ids[0, r].astype(F32), ids[1, r].astype(F32), rw[0, r], rw[1, r],
        )):
            info = jnp.where(here & (field == j), number, info)
    info_a[...] = info
    zc = [(k, j) for k in far_first(nz) for j in range(nc)] + [(0, j) for j in range(1, nc)]
    me = z * nc + c

    def there(k, j):
        return up_z(k) * nc + up_c(j)

    def zc_exchange(base, source, everything):
        return [
            send(remote(
                source.at[there(k, j)], everything.at[me],
                zs.at[base + k * nc + j], zr.at[base + k * nc + j], z=up_z(k), c=up_c(j)))
            for k, j in zc
        ]

    def from_y(k):
        return lax.rem(y - k + ny, ny)

    qa_in = zc_exchange(0, qa_send, qa_recv)
    own_a = keep(7, qa_send.at[me], qa_recv.at[me])
    info_in = [
        send(remote(info_a, info_az.at[z], zs.at[4 * nz + k], zr.at[4 * nz + k], z=up_z(k)))
        for k in far_first(nz)
    ]
    for copy in qa_in:
        copy.wait_recv()
    own_a.wait()
    own_q.wait()
    rows_a = stacked(qa_recv, nz * nc)
    part = d.ql // PAD
    for copy in wq_in:
        copy.wait_recv()
    partial = dot(rows_a, wq_all[...])
    fourth = (iota((nz * nc * PAD, 1), 0) & (PAD - 1)) == b
    last = partial[:, b * part :]
    for r in range(b):
        span = slice(r * part, (r + 1) * part)
        packed = jnp.where(fourth, pltpu.roll(last, b - r, 0), partial[:, span]).astype(BF16)
        for t in range(nz * nc):
            qp_send[t, :, span] = packed[t * PAD : (t + 1) * PAD]
    qp_in = zc_exchange(2 * nz, qp_send, qp_recv)
    own_p = keep(9, qp_send.at[me], qp_recv.at[me])
    wo_in = {
        k: send(remote(wo, wo_all.at[pl.ds(own_piece, d.rp)], ys.at[ny + k], yr.at[ny + k], y=up_y(k)))
        for k in far_first(ny)
    }
    own_o = keep(6, wo, wo_all.at[pl.ds(own_piece, d.rp)])
    wo_fwd = [send(remote(wo, wo_all.at[pl.ds(own_piece, d.rp)], cs.at[0], cr.at[0], c=other))]
    ta_in = [
        send(remote(ta_send.at[up_z(k)], ta_recv.at[z], zs.at[5 * nz + k], zr.at[5 * nz + k], z=up_z(k)))
        for k in far_first(nz)
    ]
    own_t = keep(8, ta_send.at[z], ta_recv.at[z])

    for copy in info_in:
        copy.wait_recv()
    info = info_a[...]
    for k in range(1, nz):
        info = info + info_az[up_z(k)]
    info_by[y] = info
    info_b[...] = info
    info_y_in = [
        send(remote(info_b, info_by.at[y], ys.at[2 * ny + k], yr.at[2 * ny + k], y=up_y(k)))
        for k in far_first(ny)
    ]
    loads[0].wait()
    loads[1].wait()

    own_p.wait()
    q = qp_recv[me].astype(F32)
    for (k, j), copy in zip(zc, qp_in):
        copy.wait_recv()
        q = q + qp_recv[lax.rem(z - k + nz, nz) * nc + lax.rem(c - j + nc, nc)].astype(F32)
    last = [q[b : b + 1, r * part : (r + 1) * part] for r in range(b)]
    last = jnp.concatenate(last + [jnp.zeros((PAD - b, part), F32)], axis=0)
    q = jnp.concatenate([q, last], axis=1)
    mixed = attention(d, q, kbuf, vbuf, lens, hoff)
    mx_send[...] = mixed
    mx_in = [
        send(remote(mx_send, mx_recv.at[z], zs.at[6 * nz + k], zr.at[6 * nz + k], z=up_z(k)))
        for k in far_first(nz)
    ]
    own_m = keep(10, mx_send, mx_recv.at[z])

    for copy in info_y_in:
        copy.wait_recv()
    info_c_in = send(remote(info_by, info_cc, cs.at[ny], cr.at[ny], c=other))

    for k in near_first(ny):
        wo_in[k].wait_recv()
        part = wo_all.at[pl.ds(pl.multiple_of((from_y(k) * nc + c) * d.rp, 8), d.rp)]
        wo_fwd.append(send(remote(part, part, cs.at[k], cr.at[k], c=other)))
    pick_t = iota((line, nz * PAD), 0)
    pick_s = iota((line, nz * PAD), 1)
    within = pick_s & (PAD - 1)
    pick = onehot((within < b) & ((pick_s >> (PAD.bit_length() - 1)) * b + within == pick_t))
    for copy in ta_in:
        copy.wait_recv()
    own_t.wait()
    tok = dot(pick, stacked(ta_recv, nz))
    count = float(ny * nc)
    own_ids = info_b[...][0:1, :line]
    zone = iota((8, line), 0).astype(F32) * count
    bound = onehot((own_ids >= zone) & (own_ids < zone + count))
    bound_rank = dot(bound, onehot(iota((line, line), 0) < iota((line, line), 1)))
    wide_rows = nz * SLOTS // 2
    widen = onehot((iota((wide_rows, 8), 0) >> 3) == iota((wide_rows, 8), 1))
    bound = dot(widen, bound) > 0.5
    bound_rank = dot(widen, bound_rank.astype(BF16))
    number = (iota((wide_rows, line), 0) & 7).astype(F32)
    pack_all = jnp.concatenate(
        [onehot(bound & (bound_rank == number)), onehot(bound & (bound_rank == number + 8.0))], axis=0)
    moved = dot(pack_all, tok.astype(BF16))
    for t, part in enumerate(side_by_side(d, moved[:wide_rows], moved[wide_rows:])):
        tk_all[t] = part.reshape(nz, SLOTS // 2, 128)
    tk_in = [
        send(remote(tk_all.at[x, up_z(k)], tk_recv.at[z], zs.at[9 * nz + k], zr.at[9 * nz + k], z=up_z(k)))
        for k in far_first(nz)
    ]
    own_tk = keep(0, tk_all.at[x, z], tk_recv.at[z])
    pack_all = dot(pack_all, pick).astype(BF16)
    for t in range(nx):
        gains[t] = jnp.concatenate(
            [egain[:, u * d.zb + t * 64 : u * d.zb + t * 64 + 64] for u in range(nz)], axis=1)
    for copy in wo_fwd:
        copy.wait_recv()
    own_o.wait()
    for copy in mx_in:
        copy.wait_recv()
    own_m.wait()
    all_mixed = stacked(mx_recv, nz)
    moved = dot(dot(pack_all, all_mixed).astype(BF16), wo_all[...], ((1,), (1,)))
    for t, part in enumerate(side_by_side(d, moved[:wide_rows], moved[wide_rows:])):
        f_send[t] = part.reshape(nz, SLOTS // 2, 128)
    f_in = [
        send(remote(
            f_send.at[up_x(j), up_z(k)], f_recv.at[x, z],
            fs.at[k * nx + j], fr.at[k * nx + j], x=up_x(j), z=up_z(k)))
        for k in far_first(nz) + [0] for j in far_first(nx) + [0] if k or j
    ]
    own_f = keep(1, f_send.at[x, z], f_recv.at[x, z])
    tight = dot(pick, all_mixed).astype(BF16)
    pt_send[...] = dot(tight, wo_all[...], ((1,), (1,))).astype(BF16)

    away = remote(pt_send, pt_recv.at[x], xs.at[0], xr.at[x], x=home)
    own_lanes = pl.multiple_of(lax.rem(z, d.nb) * d.zb, d.zb)
    own_block = line_rows.at[:, pl.ds(own_lanes, d.zb)]
    own_b = pltpu.make_async_copy(rb_send, own_block, load_sem.at[11])

    def to_line(k):
        return remote(
            rb_send, own_block, zs.at[7 * nz + k], zr.at[7 * nz + lax.rem(z, d.nb)], z=up_z(k))

    @pl.when(x != home)
    def _():
        away.start()

    info_c_in.wait_recv()
    near = [info_by[t] for t in range(ny)]
    far = [info_cc[t] for t in range(ny)]
    info = jnp.concatenate(
        [jnp.where(c == 0, u, v)[:, :line] for u, v in zip(near, far)]
        + [jnp.where(c == 0, v, u)[:, :line] for u, v in zip(near, far)], axis=1)
    info_out[...] = info
    id0 = info[0:1]
    id1 = info[1:2]
    low = z.astype(F32) * count
    half_width = ny * line

    def line_of(places):
        return jnp.floor((places.astype(F32) + 0.5) * (1.0 / line))

    token_line = line_of(iota((1, d.nt), 1))
    token_half = jnp.where(token_line >= ny, 1.0, 0.0)
    ours = token_half == c.astype(F32)
    staying = (id0 >= low) & (id0 < low + count)
    stay = jnp.where(staying, 1.0, 0.0)
    hits = []
    for j in range(nc):
        expert = low + (y * nc + j).astype(F32)
        hits.append((jnp.where(id0 == expert, 1.0, 0.0), jnp.where(id1 == expert, 1.0, 0.0)))
    first, second = iota((d.nt, d.nt), 0), iota((d.nt, d.nt), 1)
    earlier = first < second
    same_line = line_of(first) == line_of(second)
    same_half = (first < half_width) == (second < half_width)
    line_rank = dot(jnp.broadcast_to(stay, (8, d.nt)).astype(BF16), onehot(earlier & same_line))[0:1]
    hit_rows = jnp.concatenate([h0 + h1 for h0, h1 in hits], axis=0)
    hit_rank = dot(hit_rows.astype(BF16), onehot(earlier & same_half))
    numbers = iota((SLOTS, d.nt), 0).astype(F32)
    chosen = [
        onehot((numbers == hit_rank[j : j + 1]) & (hit_rows[j : j + 1] > 0.5) & ours) for j in range(nc)
    ]
    routes = [h0 * info[2:3] + h1 * info[3:4] for h0, h1 in hits]
    slot_route = jnp.concatenate([
        jnp.sum(chosen[j].astype(F32) * routes[j], axis=1, keepdims=True) for j in range(nc)], axis=0)
    chosen = jnp.concatenate(chosen, axis=0)
    kept = ny * SLOTS
    place = (token_line - c.astype(F32) * ny) * SLOTS + line_rank
    packed = onehot(
        (iota((kept, d.nt), 0).astype(F32) == place) & staying & ours & (line_rank < SLOTS - 0.5))
    chosen_tokens = chosen
    chosen = dot(chosen, packed, ((1,), (1,))).astype(BF16)
    owner_s = iota((ny * nz * PAD, d.nt), 0)
    owner_t = iota((ny * nz * PAD, d.nt), 1) - c * half_width
    r_of = owner_s & (PAD - 1)
    owner_i = owner_s >> (PAD.bit_length() - 1)
    first_of = (owner_i & (ny - 1)) * line + (owner_i >> (ny.bit_length() - 1)) * b
    owners = onehot((r_of < b) & (first_of + r_of == owner_t))
    owners = dot(owners, chosen_tokens, ((1,), (1,)))
    homes = []
    for r in range(b):
        last = onehot((r_of == b) & (first_of + r == owner_t))
        last = dot(last, chosen_tokens, ((1,), (1,)))
        homes.append(jnp.concatenate([owners, last], axis=1).astype(BF16))
    expert = iota((d.experts, d.nt), 0).astype(F32)
    named = onehot((id0 == expert) | (id1 == expert))
    group_t = iota((d.nt, 128), 0)
    group_g = iota((d.nt, 128), 1)
    halves = dot(named, onehot((group_t >= half_width) == (group_g > 0)))
    zone = iota((8, d.nt), 0).astype(F32) * count
    lines = dot(onehot((id0 >= zone) & (id0 < zone + count)), onehot(line_of(group_t) == group_g.astype(F32)))
    most = jnp.maximum(jnp.max(halves), jnp.max(lines))
    most_out[0] = jnp.where(most > SLOTS, 1, 0)

    own_tk.wait()
    for copy in tk_in:
        copy.wait_recv()
    own_f.wait()
    for copy in f_in:
        copy.wait_recv()
    summed = []
    for u in range(nz):
        total = tk_recv[u].astype(F32)
        for t in range(nx):
            total = total + f_recv[t, u].astype(F32)
        summed.append(total)
    low_lanes = iota((SLOTS // 2, 128), 1) < 64
    for u in range(0, nz, 2):
        span = slice(u * 64, u * 64 + 128)
        own_send[:, span] = jnp.concatenate([
            jnp.where(low_lanes, summed[u], turned(summed[u + 1])),
            jnp.where(low_lanes, turned(summed[u]), summed[u + 1])], axis=0).astype(BF16)
    own_slots = pl.ds(pl.multiple_of(y * SLOTS, SLOTS), SLOTS)
    rows_in = [
        send(remote(own_send, rows.at[own_slots], ys.at[3 * ny + k], yr.at[3 * ny + k], y=up_y(k)))
        for k in far_first(ny)
    ]
    own_s = keep(13, own_send, rows.at[own_slots])
    @pl.when(x == home)
    def _():
        total = tok + pt_send[...].astype(F32)
        for k in range(1, nx):
            source = lax.rem(x + k, nx)
            remote(pt_send, pt_recv.at[source], xs.at[0], xr.at[source], x=source).wait_recv()
            total = total + pt_recv[source].astype(F32)
        rb_send[...] = total.astype(BF16)
        own_b.start()
        for k in far_first(nz):
            to_line(k).start()

    own_s.wait()
    for copy in rows_in:
        copy.wait_recv()

    s_send[...] = dot(chosen, rows[...]).astype(BF16).reshape(nc, SLOTS, d.xs)
    xc = [(k, j) for k in far_first(nx) for j in range(nc)] + [(0, j) for j in range(1, nc)]
    our_slots = pl.ds(pl.multiple_of(c * SLOTS, SLOTS), SLOTS)
    s_in = [
        send(remote(
            s_send.at[up_c(j)], s_recv.at[x, our_slots],
            xs.at[1 + k * nc + j], xr.at[nx + k * nc + j], x=up_x(k), c=up_c(j)))
        for k, j in xc
    ]
    own_s = keep(5, s_send.at[c], s_recv.at[x, our_slots])
    for copy in loads[2:]:
        copy.wait()
    gated = jnp.zeros((nc * SLOTS, d.ff), F32)
    upward = jnp.zeros((nc * SLOTS, d.ff), F32)
    square = jnp.zeros((nc * SLOTS, 1), F32)
    waiting = dict(zip(xc, s_in))
    own_s.wait()
    for k in [0] + near_first(nx):
        for j in range(nc):
            if k or j:
                waiting[(k, j)].wait_recv()
        t = lax.rem(x - k + nx, nx)
        part = s_recv[t].astype(F32)
        square = square + jnp.sum(part * part, axis=1, keepdims=True)
        part = (part * gains[t]).astype(BF16)
        gated = gated + dot(part, gbuf[t].reshape(d.xs, d.ff))
        upward = upward + dot(part, ubuf[t].reshape(d.xs, d.ff))
    scale = lax.rsqrt(square / d.width + 1e-06)
    gated = gated * scale
    hidden = (gated / (1.0 + jnp.exp(-gated)) * (upward * scale)).astype(BF16)

    def to_half(j):
        return pl.ds(pl.multiple_of(up_c(j) * SLOTS, SLOTS), SLOTS)

    h_in = []
    for k in far_first(nx) + [0]:
        h_send[up_x(k)] = dot(hidden, dbuf[up_x(k)]).astype(BF16)
        for j in range(nc):
            if k or j:
                h_in.append(send(remote(
                    h_send.at[up_x(k), to_half(j)], h_recv.at[x, our_slots],
                    xs.at[1 + nx * nc + k * nc + j], xr.at[nx + nx * nc + k * nc + j],
                    x=up_x(k), c=up_c(j))))
    own_h = keep(6, h_send.at[x, our_slots], h_recv.at[x, our_slots])
    own_h.wait()
    for copy in h_in:
        copy.wait_recv()
    total = h_recv[0].astype(F32)
    for t in range(1, nx):
        total = total + h_recv[t].astype(F32)
    answer = total.astype(BF16).astype(F32) * slot_route
    part = d.xs // PAD
    pairs = [
        jnp.concatenate([answer[:, r * part : (r + 1) * part], answer[:, b * part :]], axis=0).astype(BF16)
        for r in range(b)
    ]

    def give(t, k):
        return remote(
            y_send.at[t * ny + up_y(k)], y_recv.at[y * nz + z],
            gs.at[t * ny + k], gr.at[z * ny + k], z=t, y=up_y(k))

    some = nz // 2
    for first_z in range(0, nz, some):
        area = slice(first_z * ny, (first_z + some) * ny)
        for r in range(b):
            from_home = homes[r][area.start * PAD : area.stop * PAD]
            y_send[area, :, r * part : (r + 1) * part] = (
                dot(from_home, pairs[r]).reshape(some * ny, PAD, part).astype(BF16))
        for t in range(first_z, first_z + some):
            for k in far_first(ny):
                send(give(t, k))

            @pl.when(z != t)
            def _():
                give(t, 0).start()

    given = nz * (ny - 1)
    own_y = keep(7, y_send.at[z * ny + y], y_recv.at[y * nz + z])
    for j in range(d.nb):
        source = x * d.nb + j

        @pl.when(z != source)
        def _():
            block = line_rows.at[:, pl.ds(j * d.zb, d.zb)]
            remote(rb_send, block, zs.at[0], zr.at[7 * nz + j], z=source).wait_recv()

    @pl.when(x == home)
    def _():
        own_b.wait()

    save = keep(12, line_rows, line_out)
    mine_t = iota((8, line), 1)
    mine_r = iota((8, line), 0)
    resid = dot(onehot((mine_r < b) & (mine_t == mine_r + z * b)), line_rows[...])
    save.wait()

    @pl.when(x != home)
    def _():
        away.wait_send()

    @pl.when(x == home)
    def _():
        for k in near_first(nz):
            to_line(k).wait_send()

    for copy in pending[:-given]:
        copy.wait_send()
    own_y.wait()
    total = jnp.zeros((PAD, part * b), F32)
    for t in range(nz):
        for k in near_first(ny):
            remote(
                y_send.at[0], y_recv.at[from_y(k) * nz + t], gs.at[0], gr.at[t * ny + k],
                z=t, y=from_y(k)).wait_recv()

        @pl.when(z != t)
        def _():
            remote(
                y_send.at[0], y_recv.at[y * nz + t], gs.at[0], gr.at[t * ny], z=t).wait_recv()
        arrived = [y_recv[u * nz + t].astype(F32) for u in range(ny)]
        while len(arrived) > 1:
            arrived = [sum(arrived[u : u + 2]) for u in range(0, len(arrived), 2)]
        total = total + arrived[0]

    last = jnp.concatenate([total[b : b + 1, r * part : (r + 1) * part] for r in range(b)], axis=0)
    out[...] = (resid[0:b] + jnp.concatenate([total[0:b], last], axis=1)).astype(BF16)
    for t in range(nz):
        @pl.when(z != t)
        def _():
            give(t, 0).wait_send()

    for copy in pending[-given:]:
        copy.wait_send()


def layer(d, args):
    def vmem(*shape, dtype=BF16):
        return pltpu.VMEM(shape, dtype)

    line = d.nz * d.b
    dma = pltpu.SemaphoreType.DMA
    inside = pl.BlockSpec(memory_space=pltpu.VMEM)
    outside = pl.BlockSpec(memory_space=pltpu.HBM)
    return pl.pallas_call(
        functools.partial(kernel, d),
        out_shape=(
            pltpu.VMEM((d.b, d.xs), BF16),
            jax.ShapeDtypeStruct((line, d.xs), BF16),
            pltpu.VMEM((4, d.nt), F32),
            pltpu.SMEM((1,), jnp.int32),
        ),
        in_specs=[outside] * 14,
        out_specs=(inside, outside, inside, pl.BlockSpec(memory_space=pltpu.SMEM)),
        scratch_shapes=[
            vmem(d.b, d.width), vmem(1, d.width, dtype=F32), vmem(d.rp, d.ql), vmem(d.rp, d.ql),
            vmem(1, d.width, dtype=F32),
            pltpu.SMEM((d.b,), jnp.int32), pltpu.SMEM((d.ql // d.hd,), F32),
            pltpu.SMEM((2, d.b), jnp.int32), pltpu.SMEM((2, d.b), F32),
            vmem(d.b, d.cache, d.hd), vmem(d.b, d.cache, d.hd),
            vmem(d.nx, d.nz, d.zb // d.nx, d.ff), vmem(d.nx, d.nz, d.zb // d.nx, d.ff), vmem(d.nx, d.ff, d.xs),
            dma((25 + 3 * d.nx,)),
            vmem(d.nz, PAD, d.zb), vmem(d.nz, PAD, d.zb),
            vmem(d.nz * d.nc, PAD, d.zb // d.nc), vmem(d.nz * d.nc, PAD, d.zb // d.nc),
            vmem(d.ny * d.rp, d.ql), vmem(d.zb, d.ql),
            vmem(d.nz * d.nc, PAD, d.ql // PAD * d.b), vmem(d.nz * d.nc, PAD, d.ql // PAD * d.b),
            vmem(PAD, d.ql), vmem(d.nz, PAD, d.ql),
            vmem(d.nx, d.nz, SLOTS // 2, 128), vmem(d.nz, SLOTS // 2, 128),
            vmem(d.nx, d.nz, SLOTS // 2, 128), vmem(d.nx, d.nz, SLOTS // 2, 128),
            vmem(d.nx, 1, d.xs, dtype=F32),
            vmem(line, d.zb), vmem(d.nx, line, d.zb), vmem(line, d.zb),
            vmem(line, d.xs), vmem(SLOTS, d.xs), vmem(d.ny * SLOTS, d.xs),
            vmem(d.nc, SLOTS, d.xs), vmem(d.nx, d.nc * SLOTS, d.xs),
            vmem(d.nx, d.nc * SLOTS, d.xs), vmem(d.nx, d.nc * SLOTS, d.xs),
            vmem(d.ny * d.nz, PAD, d.xs // PAD * d.b), vmem(d.ny * d.nz, PAD, d.xs // PAD * d.b),
            vmem(4, 128, dtype=F32), vmem(d.nz, 4, 128, dtype=F32), vmem(4, 128, dtype=F32),
            vmem(d.ny, 4, 128, dtype=F32), vmem(d.ny, 4, 128, dtype=F32),
            dma((10 * d.nz,)), dma((10 * d.nz,)),
            dma((5 * d.ny,)), dma((5 * d.ny,)),
            dma((1 + 2 * d.nx * d.nc,)), dma((d.nx + 2 * d.nx * d.nc,)),
            dma((d.ny + 1,)), dma((d.ny + 1,)),
            dma((d.nz * d.nx,)), dma((d.nz * d.nx,)),
            dma((d.nz * d.ny,)), dma((d.nz * d.ny,)),
        ],
        compiler_params=pltpu.CompilerParams(
            collective_id=0, has_side_effects=True, vmem_limit_bytes=60 * 1024 * 1024),
    )(*args)


def crowded(d, line, info, expert_gain, gate_weight, up_weight, down_weight):
    places = ("c", "y")
    copies = jnp.broadcast_to(line, (d.nc * d.ny, *line.shape))
    lines = lax.all_to_all(copies, places, split_axis=0, concat_axis=0, tiled=True)
    rows = lines.reshape(d.nt, d.xs)
    copies = jnp.broadcast_to(rows, (d.nx, *rows.shape))
    spans = lax.all_to_all(copies, "x", split_axis=0, concat_axis=0, tiled=True)
    full = jnp.moveaxis(spans, 0, 1).reshape(d.nt, d.width)
    wide = full.astype(F32)
    scale = lax.rsqrt(jnp.mean(wide * wide, axis=-1, keepdims=True) + 1e-06)
    normed = (wide * scale * expert_gain).astype(BF16)
    gated = jnp.dot(normed, gate_weight, preferred_element_type=F32)
    upward = jnp.dot(normed, up_weight, preferred_element_type=F32)
    hidden = (jax.nn.silu(gated) * upward).astype(BF16)
    term = jnp.dot(hidden, down_weight, preferred_element_type=F32).astype(BF16)
    tiles = jnp.moveaxis(term.reshape(d.nt, d.nx, d.xs), 1, 0)
    terms = lax.all_to_all(tiles, "x", split_axis=0, concat_axis=0, tiled=True)
    answer = terms.astype(F32).sum(axis=0).astype(BF16).astype(F32)
    mine = lax.axis_index(EP).astype(F32)
    route = jnp.where(info[0] == mine, info[2], 0.0) + jnp.where(info[1] == mine, info[3], 0.0)
    answer = answer * route[:, None]
    answer = answer.reshape(d.nc, d.ny, d.nz, d.b, d.xs).transpose(2, 1, 0, 3, 4)
    answer = answer.reshape(-1, d.b, d.xs)
    back = lax.all_to_all(answer, EP, split_axis=0, concat_axis=0, tiled=True)
    z, y, c = (lax.axis_index(name) for name in EP)
    first = ((c * d.ny + y) * d.nz + z) * d.b
    resid = lax.dynamic_slice_in_dim(rows, first, d.b, 0)
    return (resid.astype(F32) + back.sum(axis=0)).astype(BF16)


def local(
    tokens,
    mixer_gain,
    query_weight,
    key_cache,
    value_cache,
    seq_lengths,
    head_offset,
    output_weight,
    expert_gain,
    expert_ids,
    route_weight,
    gate_weight,
    up_weight,
    down_weight,
):
    nz, ny, nc, nx = (lax.axis_size(name) for name in ("z", "y", "c", "x"))
    batch, width = tokens.shape
    d = SimpleNamespace(
        nz=nz, ny=ny, nc=nc, nx=nx, b=batch, width=width, zb=width // nz, xs=width // nx,
        nb=nz // nx, rp=query_weight.shape[0], ql=query_weight.shape[1], hd=key_cache.shape[3],
        cache=key_cache.shape[1], ff=gate_weight.shape[2], nt=nz * ny * nc * batch,
        experts=nz * ny * nc,
    )
    done, line, info, most = layer(d, (
        tokens,
        mixer_gain.reshape(1, width),
        query_weight,
        key_cache.reshape(batch, d.cache, d.hd),
        value_cache.reshape(batch, d.cache, d.hd),
        seq_lengths,
        head_offset,
        output_weight.T,
        expert_gain.reshape(1, width),
        expert_ids.T,
        route_weight.T,
        gate_weight.reshape(nz, nx, d.zb // nx, d.ff),
        up_weight.reshape(nz, nx, d.zb // nx, d.ff),
        down_weight[0],
    ))
    return lax.cond(
        most[0] > 0,
        lambda: crowded(d, line, info, expert_gain, gate_weight[0], up_weight[0], down_weight[0]),
        lambda: done,
    )


def solution(mesh):
    split = Mesh(mesh.devices.reshape(8, 8, 2, mesh.shape["tp"]), ("z", "y", "c", "x"))
    return sharded(split)


def sharded(split):
    in_specs = (
        P(EP, None),
        P(),
        P(EP, "x"),
        P(EP, None, "x", None),
        P(EP, None, "x", None),
        P(EP),
        P("x"),
        P("x", EP),
        P(),
        P(EP, None),
        P(EP, None),
        P(EP, None, "x"),
        P(EP, None, "x"),
        P(EP, "x", None),
    )
    return jax.shard_map(local, mesh=split, in_specs=in_specs, out_specs=P(EP, "x"), check_vma=False)
```
